512 devices in a mesh: grp: 2 (over y), sp: 64 (over z, core), tp: 4 (over x).
Axes of the slice: x: 4, y: 2, z: 32, core: 2. Of those that a mesh axis runs over, the one named last changes fastest.
The devices are a block of a 4x8x32 slice.
Arguments:
- tokens: bfloat16 [32768, 2048], P(('grp', 'sp'), 'tp'), parts along dimension 0, may hold values from -6 to 6
- norm_gain: float32 [2048], replicated, may hold values from 0.1 to 1.9
- ret_query_weight: bfloat16 [2048, 256], P('sp', 'tp'), may hold values from -0.125 to 0.125
- ret_key_weight: bfloat16 [2048, 256], P('sp', 'tp'), may hold values from -0.125 to 0.125
- ret_value_weight: bfloat16 [2048, 512], P('sp', 'tp'), may hold values from -0.125 to 0.125
- fox_query_weight: bfloat16 [2048, 512], P('sp', 'tp'), may hold values from -8 to 8
- fox_key_weight: bfloat16 [2048, 512], P('sp', 'tp'), may hold values from -0.125 to 0.125
- fox_value_weight: bfloat16 [2048, 512], P('sp', 'tp'), may hold values from -0.125 to 0.125
- ret_decay: float32 [8], P('tp'), may hold values from -1 to 0, as said below
- ret_state: float32 [16, 32, 64], P(('grp', 'tp')), parts along dimension 0, may hold values from -256 to 256
- head_norm_gain: float32 [512], P('tp'), may hold values from 0.1 to 1.9
- fox_gates: float32 [32768, 8], P('grp', 'tp'), parts along dimension 0, may hold values from -49152 to 0, as said below
- ret_out_weight: bfloat16 [512, 2048], P('tp', 'sp'), may hold values from -0.1875 to 0.1875
- fox_out_weight: bfloat16 [512, 2048], P('tp', 'sp'), may hold values from -1 to 1
Outputs:
- mixed: bfloat16 [32768, 2048], P(('grp', 'sp', 'tp')), parts along dimension 0
The draws below stay inside these ranges and needn't reach their ends.
There are 2 independent parts, one for each index of `grp`. The reference program is written for one: setup_inputs(seed, part) draws one part's arguments, and reference() takes and returns one part's arrays. A program takes and returns all parts, laid end to end along the dimension named above; an argument that names none is the same for every part. Nothing has to cross between parts.
Inputs may be any that keep to these rules, and one draw needn't show every extreme that they name: `ret_decay`: each head's log decay is negative. `fox_gates`: along the positions each head's column never rises.
All inputs are finite; a program needn't handle non-finite values.
Results may differ from the reference program's by a relative error of at most 0.015.
The reference program's roundings to bfloat16 on the way count: a program that leaves them out, or rounds other values in their place, can miss the bound.
Values may be sent and summed in bfloat16 or wider, within the bound.
No kernel may reach another device: no remote copies, remote signals or barrier semaphores. Data moves between devices by JAX's collectives and lax.ppermute only.
A program may use at most 64 MiB of HBM per device.

```python
import jax
import jax.numpy as jnp
from jax import lax

D = 2048
RETAIN_HEADS = 8
DK = 32
RETAIN_VALUE_DIM = 64
FH = 8
FD = 64
TOK_DEV = 256
TOKENS = 16384
N_TP = 4


def draw_fox_query_weight(key, part):
    keys = jax.random.split(jax.random.fold_in(key, 11), 1)
    columns = FH * FD
    return (jnp.clip(jax.random.normal(keys[0], (D, columns), jnp.float32), -6.0, 6.0) * D ** (-0.5)).astype(jnp.bfloat16)


def draw_ret_decay(key, part):
    keys = jax.random.split(jax.random.fold_in(key, 23), 3)
    order = jax.random.permutation(keys[0], RETAIN_HEADS)
    quick = order < RETAIN_HEADS // 2
    quick_rate = -1.0 / jax.random.uniform(keys[1], (RETAIN_HEADS,), jnp.float32, 30.0, 100.0)
    slow_rate = -jax.random.uniform(keys[2], (RETAIN_HEADS,), jnp.float32, 0.3, 2.0) / TOKENS
    return jnp.where(quick, quick_rate, slow_rate)


def draw_ret_state(key, part):
    source = jax.random.fold_in(key, 37)
    scale = 0.2 * float(TOKENS) ** 0.5
    return scale * jnp.clip(jax.random.normal(source, (RETAIN_HEADS, DK, RETAIN_VALUE_DIM), jnp.float32), -6.0, 6.0)


def draw_fox_gates(key, part):
    keys = jax.random.split(jax.random.fold_in(key, 51), 7)
    order = jax.random.permutation(keys[0], FH)
    quick = order < FH // 2
    quick_rate = 1.0 / jax.random.uniform(keys[1], (FH,), jnp.float32, 30.0, 100.0)
    slow_rate = jax.random.uniform(keys[2], (FH,), jnp.float32, 0.5, 2.0) / TOKENS
    rates = jnp.where(quick, quick_rate, slow_rate)
    blocks = TOKENS // TOK_DEV
    factor = jnp.exp(jax.random.uniform(keys[3], (blocks, 1), jnp.float32, -0.7, 0.7))
    factor = jnp.repeat(factor, TOK_DEV, axis=0)
    jitter = jax.random.uniform(keys[4], (TOKENS, FH), jnp.float32, 0.3, 1.7)
    increments = -rates[None, :] * factor * jitter
    spots = jax.random.randint(keys[5], (3,), 0, TOKENS)
    struck = jnp.any(jnp.arange(TOKENS)[:, None] == spots[None, :], axis=1)
    losses = jax.random.uniform(keys[6], (TOKENS, FH), jnp.float32, 0.22, 0.69)
    increments = increments - jnp.where(struck[:, None], losses, 0.0)
    return jnp.cumsum(increments, axis=0)


def block_scale(own_key, extent, cuts, least, top_value):
    gain, own = 1.0, jax.random.fold_in(own_key, 6)
    for axis_at, blocks in cuts:
        heights = jnp.exp(jax.random.uniform(jax.random.fold_in(own, axis_at), (blocks,), jnp.float32, least / len(cuts), top_value / len(cuts)))
        gain = gain * jnp.repeat(heights, extent[axis_at] // blocks).reshape([-1 if axis == axis_at else 1 for axis in range(len(extent))])
    return gain


def noise(key, extent, scale, limit, cuts=(), held_as=jnp.bfloat16):
    gain = block_scale(key, extent, cuts, -0.22, 0.18) if cuts else 1.0
    entries = jax.random.normal(key, extent, jnp.float32) * scale * gain
    return jnp.minimum(jnp.maximum(entries, -limit), limit).astype(held_as)


def setup_inputs(seed: int = 0, part: int = 0) -> dict:
    key_list = jax.random.split(jax.random.key(seed), 15)
    own_keys = jax.random.split(jax.random.fold_in(key_list[14], part), 15)
    return {
        "tokens": noise(own_keys[0], (TOKENS, D), 1.0, 6.0, ((0, 64), (1, 4))),
        "norm_gain": jnp.clip(1.0 + 0.18 * jax.random.normal(key_list[1], (D,), jnp.float32), 0.1, 1.9),
        "ret_query_weight": noise(key_list[2], (D, RETAIN_HEADS * DK), D ** -0.5, 0.125, ((0, 64), (1, 4))),
        "ret_key_weight": noise(key_list[3], (D, RETAIN_HEADS * DK), D ** -0.5, 0.125, ((0, 64), (1, 4))),
        "ret_value_weight": noise(key_list[4], (D, RETAIN_HEADS * RETAIN_VALUE_DIM), D ** -0.5, 0.125, ((0, 64), (1, 4))),
        "fox_query_weight": draw_fox_query_weight(jax.random.fold_in(key_list[14], 71), part),
        "fox_key_weight": noise(key_list[6], (D, FH * FD), D ** -0.5, 0.125, ((0, 64), (1, 4))),
        "fox_value_weight": noise(key_list[7], (D, FH * FD), D ** -0.5, 0.125, ((0, 64), (1, 4))),
        "ret_decay": draw_ret_decay(jax.random.fold_in(key_list[14], 71), part),
        "ret_state": draw_ret_state(jax.random.fold_in(jax.random.fold_in(key_list[14], part), 71), part),
        "head_norm_gain": jnp.clip(1.0 + 0.18 * jax.random.normal(key_list[10], (RETAIN_HEADS * RETAIN_VALUE_DIM,), jnp.float32), 0.1, 1.9),
        "fox_gates": draw_fox_gates(jax.random.fold_in(jax.random.fold_in(key_list[14], part), 71), part),
        "ret_out_weight": noise(key_list[12], (RETAIN_HEADS * RETAIN_VALUE_DIM, D), (RETAIN_HEADS * RETAIN_VALUE_DIM + FH * FD) ** -0.5, 0.1875, ((0, 4), (1, 64))),
        "fox_out_weight": noise(key_list[13], (FH * FD, D), (FH * FD // 16) ** -0.5, 1.0, ((0, 4), (1, 64))),
    }


epsilon = 1e-06
highest = lax.Precision.HIGHEST

def head_group_norm(joined_output, norm_gains):
    center = joined_output - lax.optimization_barrier(jnp.mean(joined_output, axis=-1, keepdims=True))
    spread = lax.optimization_barrier(jnp.mean(center * center, axis=-1, keepdims=True))
    normal = center * lax.rsqrt(spread + epsilon) * norm_gains.reshape(joined_output.shape[1], joined_output.shape[2])
    return normal.reshape(joined_output.shape[0], -1).astype(jnp.bfloat16)

def retention(query_rows, key_rows, value_rows, log_decay, initial, norm_gains):
    sequence_length = query_rows.shape[0]
    blocks = sequence_length // TOK_DEV
    queries = query_rows.astype(jnp.float32).reshape(blocks, TOK_DEV, RETAIN_HEADS, DK)
    keys_all = key_rows.astype(jnp.float32).reshape(blocks, TOK_DEV, RETAIN_HEADS, DK) * DK ** (-0.5)
    values_all = value_rows.astype(jnp.float32).reshape(blocks, TOK_DEV, RETAIN_HEADS, RETAIN_VALUE_DIM)
    offsets = jnp.arange(TOK_DEV, dtype=jnp.float32)
    spread = offsets[:, None] - offsets[None, :]
    within = jnp.where(spread[None] >= 0, jnp.exp(jnp.maximum(spread, 0.0)[None] * log_decay[:, None, None]), 0.0)
    leading = jnp.exp((offsets + 1.0)[:, None] * log_decay[None, :])
    trailing = jnp.exp((TOK_DEV - 1.0 - offsets)[:, None] * log_decay[None, :])
    blockwise = jnp.exp(TOK_DEV * log_decay)

    def advance(memory, inputs):
        qblock, kblock, vblock = inputs
        scores = jnp.einsum('ihd,jhd->hij', qblock, kblock, precision=highest) * within
        inner_value = jnp.einsum('hij,jhe->ihe', scores, vblock, precision=highest)
        carried_state = jnp.einsum('ihd,hde->ihe', qblock, memory, precision=highest) * leading[:, :, None]
        summary = jnp.einsum('jhd,jhe->hde', kblock * trailing[:, :, None], vblock, precision=highest)
        return (memory * blockwise[:, None, None] + summary, inner_value + carried_state)
    _, output_rows = lax.scan(advance, initial, (queries, keys_all, values_all))
    return head_group_norm(output_rows.reshape(sequence_length, RETAIN_HEADS, RETAIN_VALUE_DIM), norm_gains)

def forgetting(query_rows, key_rows, value_rows, gates):
    sequence_length = query_rows.shape[0]
    queries = query_rows.astype(jnp.float32).reshape(sequence_length, FH, FD)
    keys_all = key_rows.astype(jnp.float32).reshape(sequence_length, FH, FD)
    values_all = value_rows.astype(jnp.float32).reshape(sequence_length, FH, FD)
    key_gates = gates.T
    key_pos = jnp.arange(sequence_length, dtype=jnp.int32)

    def block(number):
        first = (number * TOK_DEV).astype(jnp.int32)
        qblock = lax.dynamic_slice_in_dim(queries, first, TOK_DEV, 0)
        own_gates = lax.dynamic_slice_in_dim(key_gates, first, TOK_DEV, 1)
        scores = jnp.einsum('qhd,khd->hqk', qblock, keys_all) * FD ** (-0.5)
        scores = scores + own_gates[:, :, None] - key_gates[:, None, :]
        query_pos = first + jnp.arange(TOK_DEV, dtype=jnp.int32)
        scores = jnp.where(key_pos[None, None, :] <= query_pos[None, :, None], scores, -jnp.inf)
        highest_score = lax.optimization_barrier(jnp.max(scores, axis=-1, keepdims=True))
        weights = jnp.exp(scores - highest_score)
        totals = lax.optimization_barrier(jnp.sum(weights, axis=-1))
        rounded = lax.optimization_barrier(weights.astype(jnp.bfloat16)).astype(jnp.float32)
        weighted = jnp.einsum('hqk,khd->hqd', rounded, values_all)
        result = weighted / totals[:, :, None]
        return jnp.transpose(result, (1, 0, 2)).reshape(TOK_DEV, FH * FD).astype(jnp.bfloat16)
    pieces = lax.map(block, jnp.arange(sequence_length // TOK_DEV, dtype=jnp.int32))
    return pieces.reshape(sequence_length, FH * FD)

def reference(tokens, norm_gain, ret_query_weight, ret_key_weight, ret_value_weight, fox_query_weight, fox_key_weight, fox_value_weight, ret_decay, ret_state, head_norm_gain, fox_gates, ret_out_weight, fox_out_weight):
    widened = tokens.astype(jnp.float32)
    normed = (widened * lax.rsqrt(lax.optimization_barrier(jnp.mean(widened * widened, axis=-1, keepdims=True)) + epsilon) * norm_gain).astype(jnp.bfloat16)
    matrices = (ret_query_weight, ret_key_weight, ret_value_weight, fox_query_weight, fox_key_weight, fox_value_weight)
    ret_query, ret_key, ret_value, fox_query, fox_key, fox_value = [jnp.dot(normed, matrix, preferred_element_type=jnp.float32).astype(jnp.bfloat16) for matrix in matrices]
    retention_mixed = retention(ret_query, ret_key, ret_value, ret_decay, ret_state, head_norm_gain)
    fox_mix = forgetting(fox_query, fox_key, fox_value, fox_gates)
    ret_width = RETAIN_HEADS * RETAIN_VALUE_DIM // N_TP
    fox_width = FH * FD // N_TP
    summed = jnp.zeros((tokens.shape[0], D), jnp.float32)
    for member in range(N_TP):
        portion = jnp.dot(retention_mixed[:, member * ret_width:(member + 1) * ret_width], ret_out_weight[member * ret_width:(member + 1) * ret_width], preferred_element_type=jnp.float32)
        portion = portion + jnp.dot(fox_mix[:, member * fox_width:(member + 1) * fox_width], fox_out_weight[member * fox_width:(member + 1) * fox_width], preferred_element_type=jnp.float32)
        summed = summed + lax.optimization_barrier(portion.astype(jnp.bfloat16)).astype(jnp.float32)
    return summed.astype(jnp.bfloat16)
```

```python
import jax
import jax.numpy as jnp
from jax import lax
from jax.experimental import pallas as pl
from jax.experimental.pallas import tpu as pltpu
from jax.sharding import Mesh
from jax.sharding import PartitionSpec as P

SP = ("sp_0", "sp_1")
GRP_SP = ("grp", "sp_0", "sp_1")
GRP_SP_TP = ("grp", "sp_0", "sp_1", "tp")

EPSILON = 1e-06
LOG2E = 1.4426950408889634

SMALL_WEIGHT = 2.0**18
QUERY_WEIGHT = 2.0**12
FOX_OUT_WEIGHT = 2.0**15
KEY_VALUE = 2.0**7
STATE = 2.0**-9
STATE_LOW = 2.0**11


def head_norm(raw, gain):
    center = raw - jnp.mean(raw, axis=-1, keepdims=True)
    spread = jnp.mean(center * center, axis=-1, keepdims=True)
    return (center * lax.rsqrt(spread + EPSILON) * gain).astype(jnp.bfloat16)


def attention_kernel(place, query, gathered, gates, out, *, scale, value_scale):
    chunk = query.shape[0]
    width = query.shape[1]
    q = query[...]

    def logits_of(j):
        pairs = gathered[j]
        s = lax.dot_general(q, pairs, (((1,), (1,)), ((), ())), preferred_element_type=jnp.float32)
        return s * scale - gates[j], pairs

    own = place[0]
    t, pairs = logits_of(own)
    row = lax.broadcasted_iota(jnp.int32, (chunk, chunk), 0)
    col = lax.broadcasted_iota(jnp.int32, (chunk, chunk), 1)
    t = jnp.where(col <= row, t, -jnp.inf)
    top = jnp.max(t, axis=1, keepdims=True)
    p = jnp.exp2(t - top)
    total = jnp.sum(p, axis=1, keepdims=True)
    mixed = jnp.dot(p.astype(jnp.bfloat16), pairs, preferred_element_type=jnp.float32)

    def step(j, state):
        top, total, mixed = state
        t, pairs = logits_of(j)
        new = jnp.maximum(top, jnp.max(t, axis=1, keepdims=True))
        p = jnp.exp2(t - new)
        keep = jnp.exp2(top - new)
        total = total * keep + jnp.sum(p, axis=1, keepdims=True)
        mixed = mixed * keep + jnp.dot(
            p.astype(jnp.bfloat16), pairs, preferred_element_type=jnp.float32
        )
        return new, total, mixed

    _, total, mixed = lax.fori_loop(0, own, step, (top, total, mixed))
    out[...] = ((mixed * value_scale) / total)[:, width // 2 :].astype(out.dtype)


def attend(place, query, gathered, gates, scale):
    chunk, head = query.shape
    padded = jnp.concatenate([query, jnp.zeros_like(query)], axis=1)
    vmem = pl.BlockSpec(memory_space=pltpu.VMEM)
    return pl.pallas_call(
        lambda *refs: attention_kernel(
            *refs, scale=scale * LOG2E / KEY_VALUE, value_scale=1.0 / KEY_VALUE
        ),
        out_shape=jax.ShapeDtypeStruct((chunk, head), jnp.bfloat16),
        in_specs=[pl.BlockSpec(memory_space=pltpu.SMEM), vmem, vmem, vmem],
        out_specs=vmem,
        compiler_params=pltpu.CompilerParams(vmem_limit_bytes=40 * 2**20),
        name="attend",
    )(place[None], padded, gathered, gates)


def local(
    tokens,
    norm_gain,
    ret_query_weight,
    ret_key_weight,
    ret_value_weight,
    fox_query_weight,
    fox_key_weight,
    fox_value_weight,
    ret_decay,
    ret_state,
    head_norm_gain,
    fox_gates,
    ret_out_weight,
    fox_out_weight,
):
    f32, bf16, f16 = jnp.float32, jnp.bfloat16, jnp.float16
    chip, core = lax.axis_index("sp_0"), lax.axis_index("sp_1")
    chips, cores, tp = (lax.axis_size(a) for a in ("sp_0", "sp_1", "tp"))
    rows = tokens.shape[0]
    chunk = rows * cores
    swap = [(k, cores - 1 - k) for k in range(cores)]

    sent = jnp.broadcast_to(tokens[None], (cores * tp, *tokens.shape))
    arrived = lax.all_to_all(sent, ("sp_1", "tp"), 0, 0, tiled=True)
    wide = arrived.reshape(cores, tp, rows, -1).transpose(0, 2, 1, 3).reshape(chunk, -1)

    def by_head(weight, scale):
        split = weight.astype(f32).reshape(weight.shape[0], cores, -1) * scale
        return jnp.moveaxis(split, 1, 0)

    def out_by_head(weight, scale):
        split = weight.astype(f32).reshape(cores, -1, weight.shape[1]) * scale
        return jnp.swapaxes(split, 1, 2)

    sections = (
        (out_by_head, ret_out_weight, SMALL_WEIGHT),
        (out_by_head, fox_out_weight, FOX_OUT_WEIGHT),
        (by_head, fox_key_weight, SMALL_WEIGHT),
        (by_head, fox_value_weight, SMALL_WEIGHT),
        (by_head, fox_query_weight, QUERY_WEIGHT),
        (by_head, ret_value_weight, SMALL_WEIGHT),
        (by_head, ret_key_weight, SMALL_WEIGHT),
        (by_head, ret_query_weight, SMALL_WEIGHT),
    )
    pieces = [make(weight, scale) for make, weight, scale in sections]
    packed = jnp.concatenate(pieces, axis=2).astype(f16)
    packed = jnp.pad(packed, ((0, 0), (0, 0), (0, -packed.shape[2] % 128)))
    packed = lax.all_to_all(packed, "sp_1", 0, 0, tiled=True).reshape(-1, packed.shape[2])
    weights = lax.all_gather(packed, "sp_0", axis=0, tiled=True)
    back = jnp.concatenate(
        [jnp.full((p.shape[2],), 1.0 / s, f32) for p, (_, _, s) in zip(pieces, sections)]
    )
    weights = (weights[:, : back.shape[0]].astype(f32) * back).astype(bf16)
    out_width = pieces[0].shape[2] + pieces[1].shape[2]
    out_own = weights[:, :out_width]
    out_other = lax.ppermute(out_own, "sp_1", swap)

    widened = wide.astype(f32)
    normed = (
        widened
        * lax.rsqrt(jnp.mean(widened * widened, axis=-1, keepdims=True) + EPSILON)
        * norm_gain
    ).astype(bf16)
    projected = jnp.dot(normed, weights[:, out_width:], preferred_element_type=f32).astype(bf16)
    ends, at = [], 0
    for piece in pieces[2:]:
        at += piece.shape[2]
        ends.append(at)
    pair_width = ends[1]
    pairs = projected[:, :pair_width]
    _, _, fox_query, ret_value, ret_key, ret_query = jnp.split(projected, ends[:-1], axis=1)

    decay = lax.dynamic_index_in_dim(ret_decay, core, 0, False)
    key_scale = ret_key.shape[1] ** (-0.5)
    at = jnp.arange(chunk, dtype=f32)
    trailing = jnp.exp((chunk - 1.0 - at) * decay) * key_scale
    summary = lax.dot_general(
        ret_key.astype(f32) * trailing[:, None],
        ret_value.astype(f32),
        (((0,), (0,)), ((), ())),
        preferred_element_type=f32,
    )
    scaled = summary * STATE
    high = lax.reduce_precision(scaled, 5, 10)
    low = (scaled - high) * STATE_LOW
    payload = jnp.concatenate(
        [pairs.astype(f32) * KEY_VALUE, jnp.concatenate([high, low], axis=1)], axis=0
    ).astype(f16)
    gathered = lax.all_gather(payload, "sp_0", axis=0, tiled=False)

    gates = lax.dynamic_index_in_dim(fox_gates, core, 1, False)
    reference_gate = lax.dynamic_index_in_dim(gates, chip * chunk, 0, True)
    gates = ((gates - reference_gate) * LOG2E).reshape(chips, 1, chunk)
    fox_mix = attend(
        chip.astype(jnp.int32),
        fox_query,
        gathered[:, :chunk, :].astype(f32).astype(bf16),
        gates,
        fox_query.shape[1] ** (-0.5)
    )

    value_size = ret_value.shape[1]
    summaries = gathered[:, chunk:, :].astype(f32)
    summaries = summaries[:, :, :value_size] + summaries[:, :, value_size:] * (1.0 / STATE_LOW)
    ids = jnp.arange(chips, dtype=jnp.int32)
    distance = jnp.maximum(chip - ids - 1, 0).astype(f32) * chunk
    share = jnp.where(ids < chip, jnp.exp(distance * decay), 0.0) * (1.0 / STATE)
    before = jnp.sum(summaries * share[:, None, None], axis=0)
    first = (chip * chunk).astype(f32)
    state = lax.dynamic_index_in_dim(ret_state, core, 0, False)
    entering = jnp.exp(first * decay) * state + before
    spread = at[:, None] - at[None, :]
    within = jnp.where(spread >= 0, jnp.exp(jnp.maximum(spread, 0.0) * decay), 0.0) * key_scale
    near = (
        lax.dot_general(
            ret_query, ret_key, (((1,), (1,)), ((), ())), preferred_element_type=f32
        )
        * within
    )
    inner = jnp.dot(near, ret_value.astype(f32), preferred_element_type=f32)
    carried = jnp.dot(
        ret_query.astype(f32), entering, preferred_element_type=f32, precision=lax.Precision.HIGHEST
    )
    carried = carried * jnp.exp((at + 1.0) * decay)[:, None]
    gain = lax.dynamic_slice_in_dim(head_norm_gain, core * value_size, value_size)
    ret_mix = head_norm(inner + carried, gain)

    mix = jnp.concatenate([ret_mix, fox_mix], axis=1)
    mine = lax.dynamic_slice_in_dim(mix, core * rows, rows, 0)
    theirs = lax.dynamic_slice_in_dim(mix, (cores - 1 - core) * rows, rows, 0)
    other = lax.ppermute(theirs, "sp_1", swap)

    def project(rows_in, weight):
        return lax.dot_general(
            rows_in, weight, (((1,), (1,)), ((), ())), preferred_element_type=f32
        )

    partial = (project(mine, out_own) + project(other, out_other)).astype(bf16)
    blocks = partial.reshape(tp, rows // tp, -1)
    arrived = lax.all_to_all(blocks, "tp", 0, 0, tiled=True)
    return arrived.astype(f32).sum(axis=0).astype(bf16)


def solution(mesh):
    torus = Mesh(
        mesh.devices.reshape(mesh.shape["grp"], mesh.shape["sp"] // 2, 2, mesh.shape["tp"]),
        ("grp", "sp_0", "sp_1", "tp"),
    )
    return jax.shard_map(
        local,
        mesh=torus,
        in_specs=(
            P(GRP_SP, "tp"),
            P(),
            P(SP, "tp"),
            P(SP, "tp"),
            P(SP, "tp"),
            P(SP, "tp"),
            P(SP, "tp"),
            P(SP, "tp"),
            P("tp"),
            P(("grp", "tp"), None, None),
            P("tp"),
            P("grp", "tp"),
            P("tp", SP),
            P("tp", SP),
        ),
        out_specs=P(GRP_SP_TP, None),
        check_vma=False,
    )
```

```python
import jax
import jax.numpy as jnp
from jax import lax
from jax.experimental import pallas as pl
from jax.experimental.pallas import tpu as pltpu
from jax.sharding import Mesh
from jax.sharding import PartitionSpec as P


SP = ("sp_0", "sp_1")
CHIP = ("sp_1", "tp")
GRP_SP = ("grp", "sp_0", "sp_1")
GRP_SP_TP = ("grp", "sp_0", "sp_1", "tp")

EPSILON = 1e-06
LOG2E = 1.4426950408889634
MIB = 2**20

SMALL_WEIGHT = 2.0**18
QUERY_WEIGHT = 2.0**12
FOX_OUT_WEIGHT = 2.0**15
KEY_VALUE = 2.0**7
STATE = 2.0**-9
STATE_LOW = 2.0**8

VMEM = pl.BlockSpec(memory_space=pltpu.VMEM)
SMEM = pl.BlockSpec(memory_space=pltpu.SMEM)
NT = (((1,), (1,)), ((), ()))
TN = (((0,), (0,)), ((), ()))


def dot(a, b, dims=(((1,), (0,)), ((), ()))):
    return lax.dot_general(a, b, dims, preferred_element_type=jnp.float32)


def two_terms(x):
    high = x.astype(jnp.bfloat16)
    return high, (x - high.astype(jnp.float32)).astype(jnp.bfloat16)


def column_of(count):
    return lax.broadcasted_iota(jnp.int32, (count, 1), 0).astype(jnp.float32)


def pack_kernel(out_ret, out_fox, fk, fv, fq, rv, rk, rq, packed):
    f32 = jnp.float32
    heads = packed.shape[0]

    def columns(ref, h):
        size = ref.shape[1] // heads
        return ref[...].astype(f32)[:, h * size : (h + 1) * size]

    for h in range(heads):
        parts = [columns(ref, h) for ref in (out_ret, out_fox, fk, fv, fq, rv, rk, rq)]
        joined = jnp.concatenate(parts, axis=1)
        blank = packed.shape[2] - joined.shape[1]
        joined = jnp.concatenate([joined, jnp.zeros((joined.shape[0], blank), f32)], axis=1)
        packed[h] = joined.astype(packed.dtype)


def project_kernel(place, decays, tokens, gains, weights, query, values, keys, queries, payload, *, key, cores):
    f32, bf16 = jnp.float32, jnp.bfloat16
    rows, width = tokens.shape[1:]
    parts, value = tokens.shape[0] // cores, 2 * key
    for c in range(cores):
        square = jnp.zeros((rows, 1), f32)
        for k in range(parts):
            x = tokens[c * parts + k].astype(f32)
            square = square + jnp.sum(x * x, axis=1, keepdims=True)
        factor = lax.rsqrt(square * (1.0 / (parts * width)) + EPSILON)
        total = jnp.zeros((rows, weights.shape[1]), f32)
        for k in range(parts):
            x = tokens[c * parts + k].astype(f32)
            normed = (x * factor * gains[k]).astype(bf16)
            total = total + dot(normed, weights[k * width : (k + 1) * width, :])
        total = total.astype(bf16)
        at = slice(c * rows, (c + 1) * rows)
        payload[at, :] = total[:, : 2 * value].astype(f32) * KEY_VALUE
        lane = lax.broadcasted_iota(jnp.int32, (rows, 2 * value), 1)
        mixed = total[:, 2 * value : 4 * value].astype(f32)
        query[at, :] = jnp.where(lane < value, mixed, 0.0).astype(bf16)
        values[at, :] = total[:, 3 * value : 4 * value]
        keys[at, :] = total[:, 4 * value : 4 * value + key]
        queries[at, :] = total[:, 4 * value + key : 4 * value + 2 * key]
    chunk = rows * cores
    trailing = jnp.exp((chunk - 1.0 - column_of(chunk)) * decays[place[1]]) * key ** (-0.5)
    high, low = two_terms(keys[...].astype(f32) * trailing)
    summary = (dot(high, values[...], TN) + dot(low, values[...], TN)) * STATE
    high = summary.astype(bf16).astype(f32)
    payload[chunk:, :] = jnp.concatenate([high, (summary - high) * STATE_LOW], axis=1)


def mix_kernel(place, decays, query, values, keys, queries, gathered, gates, state, gains, mix, *, key):
    f32, bf16 = jnp.float32, jnp.bfloat16
    chunk, value = query.shape[0], 2 * key
    own, head = place[0], place[1]
    decay = decays[head]
    attending = query[...]
    scale = value ** (-0.5) * LOG2E / KEY_VALUE
    base = jnp.max(gates[head, own], axis=1, keepdims=True)

    def logits_of(j):
        pairs = gathered[j, :chunk, :]
        return dot(attending, pairs, NT) * scale - (gates[head, j] - base) * LOG2E, pairs

    row = lax.broadcasted_iota(jnp.int32, (chunk, chunk), 0)
    col = lax.broadcasted_iota(jnp.int32, (chunk, chunk), 1)
    t, pairs = logits_of(own)
    t = jnp.where(col <= row, t, -jnp.inf)
    top = jnp.max(t, axis=1, keepdims=True)
    p = jnp.exp2(t - top)
    total = jnp.sum(p, axis=1, keepdims=True)
    mixed = dot(p.astype(bf16), pairs)

    ones = jnp.ones((1, 2 * value), f32)
    per_chunk = jnp.exp(ones * (chunk * decay))

    def step(j, carry):
        top, total, mixed, memory = carry
        t, pairs = logits_of(j)
        new = jnp.maximum(top, jnp.max(t, axis=1, keepdims=True))
        p = jnp.exp2(t - new)
        keep = jnp.exp2(top - new)
        total = total * keep + jnp.sum(p, axis=1, keepdims=True)
        mixed = mixed * keep + dot(p.astype(bf16), pairs)
        memory = memory * per_chunk + gathered[j, chunk:, :].astype(f32)
        return new, total, mixed, memory

    memory = jnp.zeros((key, 2 * value), f32)
    _, total, mixed, memory = lax.fori_loop(0, own, step, (top, total, mixed, memory))
    fox = (mixed * (1.0 / KEY_VALUE) / total)[:, value:]

    memory = (memory[:, :value] + memory[:, value:] * (1.0 / STATE_LOW)) * (1.0 / STATE)
    first = (own * chunk).astype(f32)
    entering = jnp.exp(ones[:, :value] * (first * decay)) * state[head] + memory
    ret_query = queries[...]
    spread = (row - col).astype(f32)
    within = jnp.where(col <= row, jnp.exp(jnp.maximum(spread, 0.0) * decay), 0.0)
    near = dot(ret_query, keys[...], NT) * within * key ** (-0.5)
    high, low = two_terms(entering)
    carried = dot(ret_query, high) + dot(ret_query, low)
    raw = dot(near.astype(bf16), values[...]) + carried * jnp.exp((column_of(chunk) + 1.0) * decay)
    center = raw - jnp.mean(raw, axis=1, keepdims=True)
    variance = jnp.mean(center * center, axis=1, keepdims=True)
    ret = center * lax.rsqrt(variance + EPSILON) * gains[head]
    mix[...] = jnp.concatenate([ret, fox], axis=1).astype(bf16)


def output_kernel(mixes, weights, out, *, cores):
    parts = mixes.shape[0] // cores
    summed = jnp.zeros(out.shape, jnp.float32)
    for k in range(parts):
        partial = sum(
            dot(mixes[c * parts + k], weights[c * parts + k], NT) for c in range(cores)
        )
        summed = summed + partial.astype(jnp.bfloat16).astype(jnp.float32)
    out[...] = summed.astype(out.dtype)


def kernel(body, out_shape, in_specs, limit):
    many = isinstance(out_shape, tuple)
    return pl.pallas_call(
        body,
        out_shape=out_shape,
        in_specs=in_specs,
        out_specs=(VMEM,) * len(out_shape) if many else VMEM,
        compiler_params=pltpu.CompilerParams(vmem_limit_bytes=limit * MIB),
    )


def layer(
    tokens,
    norm_gain,
    ret_query_weight,
    ret_key_weight,
    ret_value_weight,
    fox_query_weight,
    fox_key_weight,
    fox_value_weight,
    ret_decay,
    ret_state,
    head_norm_gain,
    fox_gates,
    ret_out_weight,
    fox_out_weight,
):
    f32, bf16, f16 = jnp.float32, jnp.bfloat16, jnp.float16
    chip, core = lax.axis_index("sp_0"), lax.axis_index("sp_1")
    chips, cores, tp = (lax.axis_size(a) for a in ("sp_0", "sp_1", "tp"))
    rows, width = tokens.shape
    chunk = rows * cores
    key, value = ret_query_weight.shape[1] // cores, ret_value_weight.shape[1] // cores
    place = jnp.stack([chip, core]).astype(jnp.int32)

    sent = jnp.broadcast_to(tokens[None], (cores * tp, rows, width))
    wide = lax.all_to_all(sent, CHIP, 0, 0, tiled=True)

    shard = fox_key_weight.shape[0]
    lanes = 2 * value + 4 * value + 2 * key
    padded = lanes + -lanes % 128
    packed = pl.pallas_call(
        pack_kernel,
        out_shape=jax.ShapeDtypeStruct((cores, shard, padded), bf16),
        grid=(1,),
        in_specs=[
            pl.BlockSpec((shard, size * cores), lambda i: (0, 0))
            for size in (value,) * 6 + (key,) * 2
        ],
        out_specs=pl.BlockSpec((cores, shard, padded), lambda i: (0, 0, 0)),
        name="pack",
    )(
        ret_out_weight.T,
        fox_out_weight.T,
        fox_key_weight,
        fox_value_weight,
        fox_query_weight,
        ret_value_weight,
        ret_key_weight,
        ret_query_weight,
    )
    packed = lax.all_to_all(packed, "sp_1", 0, 0, tiled=True).reshape(-1, padded)
    widths = (value, value, value, value, value, value, key, key, padded - lanes)
    scales = (SMALL_WEIGHT, FOX_OUT_WEIGHT, SMALL_WEIGHT, SMALL_WEIGHT, QUERY_WEIGHT)
    scales += (SMALL_WEIGHT, SMALL_WEIGHT, SMALL_WEIGHT, 1.0)
    forth = jnp.concatenate([jnp.full((w,), s, f32) for w, s in zip(widths, scales)])
    weights = lax.all_gather(
        (packed.astype(f32) * forth).astype(f16), "sp_0", axis=0, tiled=True
    )
    back = 1.0 / forth
    out_weight = (weights[:, : 2 * value].astype(f32) * back[: 2 * value]).astype(bf16)
    in_weight = (
        weights[:, 2 * value : lanes].astype(f32) * back[2 * value : lanes]
    ).astype(bf16)

    *parts, payload = kernel(
        lambda *refs: project_kernel(*refs, key=key, cores=cores),
        (
            jax.ShapeDtypeStruct((chunk, 2 * value), bf16),
            jax.ShapeDtypeStruct((chunk, value), bf16),
            jax.ShapeDtypeStruct((chunk, key), bf16),
            jax.ShapeDtypeStruct((chunk, key), bf16),
            jax.ShapeDtypeStruct((chunk + key, 2 * value), f32),
        ),
        [SMEM, SMEM, VMEM, VMEM, VMEM],
        20,
    )(place, ret_decay, wide, norm_gain.reshape(tp, 1, width), in_weight)

    sent = jnp.broadcast_to(out_weight[None], (cores * tp, *out_weight.shape))
    out_weights = lax.all_to_all(sent, CHIP, 0, 0, tiled=True)

    gathered = lax.all_gather(payload.astype(f16), "sp_0", axis=0, tiled=False)
    gathered = gathered.astype(f32).astype(bf16)

    mix = kernel(
        lambda *refs: mix_kernel(*refs, key=key),
        jax.ShapeDtypeStruct((chunk, 2 * value), bf16),
        [SMEM, SMEM] + [VMEM] * 8,
        24,
    )(
        place,
        ret_decay,
        *parts,
        gathered,
        fox_gates.T.reshape(cores, chips, 1, chunk),
        ret_state,
        head_norm_gain.reshape(cores, 1, value),
    )

    final = rows // tp
    mixes = lax.all_to_all(mix.reshape(cores * tp, final, -1), CHIP, 0, 0, tiled=True)
    return kernel(
        lambda *refs: output_kernel(*refs, cores=cores),
        jax.ShapeDtypeStruct((final, out_weight.shape[0]), bf16),
        [VMEM, VMEM],
        16,
    )(mixes, out_weights)


def solution(mesh):
    torus = Mesh(
        mesh.devices.reshape(mesh.shape["grp"], mesh.shape["sp"] // 2, 2, mesh.shape["tp"]),
        ("grp", "sp_0", "sp_1", "tp"),
    )
    return jax.shard_map(
        layer,
        mesh=torus,
        in_specs=(
            P(GRP_SP, "tp"),
            P(),
            P(SP, "tp"),
            P(SP, "tp"),
            P(SP, "tp"),
            P(SP, "tp"),
            P(SP, "tp"),
            P(SP, "tp"),
            P("tp"),
            P(("grp", "tp"), None, None),
            P("tp"),
            P("grp", "tp"),
            P("tp", SP),
            P("tp", SP),
        ),
        out_specs=P(GRP_SP_TP, None),
        check_vma=False,
    )
```

```python
import jax
import jax.numpy as jnp
from jax import lax
from jax.experimental import pallas as pl
from jax.experimental.pallas import tpu as pltpu
from jax.sharding import Mesh
from jax.sharding import PartitionSpec as P


SP = ("sp_0", "sp_1")
CHIP = ("sp_1", "tp")
GRP_SP = ("grp", "sp_0", "sp_1")
GRP_SP_TP = ("grp", "sp_0", "sp_1", "tp")

EPSILON = 1e-06
LOG2E = 1.4426950408889634
MIB = 2**20

SMALL_WEIGHT = 2.0**18
QUERY_WEIGHT = 2.0**12
FOX_OUT_WEIGHT = 2.0**15
KEY_VALUE = 2.0**7
STATE = 2.0**-9
STATE_LOW = 2.0**8

VMEM = pl.BlockSpec(memory_space=pltpu.VMEM)
SMEM = pl.BlockSpec(memory_space=pltpu.SMEM)
HBM = pl.BlockSpec(memory_space=pltpu.HBM)
NT = (((1,), (1,)), ((), ()))
TN = (((0,), (0,)), ((), ()))


def dot(a, b, dims=(((1,), (0,)), ((), ()))):
    return lax.dot_general(a, b, dims, preferred_element_type=jnp.float32)


def two_terms(x):
    high = x.astype(jnp.bfloat16)
    return high, (x - high.astype(jnp.float32)).astype(jnp.bfloat16)


def column_of(count):
    return lax.broadcasted_iota(jnp.int32, (count, 1), 0).astype(jnp.float32)


def copies(source, target, signals):
    return [
        pltpu.make_async_copy(source, target.at[k], signals.at[k]) for k in range(target.shape[0])
    ]


def pack_kernel(tokens, out_ret, out_fox, fk, fv, fq, rv, rk, rq, packed, sent, signals):
    f32 = jnp.float32
    heads = packed.shape[0]
    started = copies(tokens, sent, signals)
    for copy in started:
        copy.start()

    def columns(ref, h):
        size = ref.shape[1] // heads
        return ref[...].astype(f32)[:, h * size : (h + 1) * size]

    for h in range(heads):
        parts = [columns(ref, h) for ref in (out_ret, out_fox, fk, fv, fq, rv, rk, rq)]
        joined = jnp.concatenate(parts, axis=1)
        blank = packed.shape[2] - joined.shape[1]
        joined = jnp.concatenate([joined, jnp.zeros((joined.shape[0], blank), f32)], axis=1)
        packed[h] = joined.astype(packed.dtype)
    for copy in started:
        copy.wait()


def project_kernel(
    place,
    decays,
    tokens,
    gains,
    stored,
    back,
    query,
    values,
    keys,
    queries,
    payload,
    sent,
    weights,
    arrived,
    signals,
    *,
    key,
    cores,
):
    f32, bf16 = jnp.float32, jnp.bfloat16
    rows, width = tokens.shape[1:]
    parts, value = tokens.shape[0] // cores, 2 * key
    first, last = 2 * value, 6 * value + 2 * key
    reading = pltpu.make_async_copy(stored, weights, arrived)
    reading.start()
    factors = []
    for c in range(cores):
        square = jnp.zeros((rows, 1), f32)
        for k in range(parts):
            x = tokens[c * parts + k].astype(f32)
            square = square + jnp.sum(x * x, axis=1, keepdims=True)
        factors.append(lax.rsqrt(square * (1.0 / (parts * width)) + EPSILON))
    reading.wait()
    started = copies(weights.at[:, :first], sent, signals)
    for copy in started:
        copy.start()
    for c in range(cores):
        total = jnp.zeros((rows, last - first), f32)
        for k in range(parts):
            x = tokens[c * parts + k].astype(f32)
            normed = (x * factors[c] * gains[k]).astype(bf16)
            total = total + dot(normed, weights[k * width : (k + 1) * width, first:last])
        total = (total * back[:, first:last]).astype(bf16)
        at = slice(c * rows, (c + 1) * rows)
        payload[at, :] = total[:, : 2 * value].astype(f32) * KEY_VALUE
        lane = lax.broadcasted_iota(jnp.int32, (rows, 2 * value), 1)
        mixed = total[:, 2 * value : 4 * value].astype(f32)
        query[at, :] = jnp.where(lane < value, mixed, 0.0).astype(bf16)
        values[at, :] = total[:, 3 * value : 4 * value]
        keys[at, :] = total[:, 4 * value : 4 * value + key]
        queries[at, :] = total[:, 4 * value + key : 4 * value + 2 * key]
    chunk = rows * cores
    trailing = jnp.exp((chunk - 1.0 - column_of(chunk)) * decays[place[1]]) * key ** (-0.5)
    high, low = two_terms(keys[...].astype(f32) * trailing)
    summary = (dot(high, values[...], TN) + dot(low, values[...], TN)) * STATE
    high = summary.astype(bf16).astype(f32)
    payload[chunk:, :] = jnp.concatenate([high, (summary - high) * STATE_LOW], axis=1)
    for copy in started:
        copy.wait()


def mix_kernel(place, decays, query, values, keys, queries, gathered, gates, state, gains, mix, *, key):
    f32, bf16 = jnp.float32, jnp.bfloat16
    chunk, value = query.shape[0], 2 * key
    own, head = place[0], place[1]
    decay = decays[head]
    attending = query[...]
    scale = value ** (-0.5) * LOG2E / KEY_VALUE

    def gates_of(j):
        pair = gates[:, pl.ds(pl.multiple_of(j * chunk, chunk), chunk)]
        return jnp.where(head == 0, pair[:1], pair[1:])

    base = jnp.max(gates_of(own), axis=1, keepdims=True)

    def logits_of(j):
        pairs = gathered[j, :chunk, :]
        return dot(attending, pairs, NT) * scale - (gates_of(j) - base) * LOG2E, pairs

    row = lax.broadcasted_iota(jnp.int32, (chunk, chunk), 0)
    col = lax.broadcasted_iota(jnp.int32, (chunk, chunk), 1)
    t, pairs = logits_of(own)
    t = jnp.where(col <= row, t, -jnp.inf)
    top = jnp.max(t, axis=1, keepdims=True)
    p = jnp.exp2(t - top)
    total = jnp.sum(p, axis=1, keepdims=True)
    mixed = dot(p.astype(bf16), pairs)

    ones = jnp.ones((1, 2 * value), f32)
    per_chunk = jnp.exp(ones * (chunk * decay))

    def step(j, carry):
        top, total, mixed, memory = carry
        t, pairs = logits_of(j)
        new = jnp.maximum(top, jnp.max(t, axis=1, keepdims=True))
        p = jnp.exp2(t - new)
        keep = jnp.exp2(top - new)
        total = total * keep + jnp.sum(p, axis=1, keepdims=True)
        mixed = mixed * keep + dot(p.astype(bf16), pairs)
        memory = memory * per_chunk + gathered[j, chunk:, :].astype(f32)
        return new, total, mixed, memory

    memory = jnp.zeros((key, 2 * value), f32)
    _, total, mixed, memory = lax.fori_loop(0, own, step, (top, total, mixed, memory))
    fox = (mixed * (1.0 / KEY_VALUE) / total)[:, value:]

    memory = (memory[:, :value] + memory[:, value:] * (1.0 / STATE_LOW)) * (1.0 / STATE)
    first = (own * chunk).astype(f32)
    entering = jnp.exp(ones[:, :value] * (first * decay)) * state[head] + memory
    ret_query = queries[...]
    spread = (row - col).astype(f32)
    within = jnp.where(col <= row, jnp.exp(jnp.maximum(spread, 0.0) * decay), 0.0)
    near = dot(ret_query, keys[...], NT) * within * key ** (-0.5)
    high, low = two_terms(entering)
    carried = dot(ret_query, high) + dot(ret_query, low)
    raw = dot(near.astype(bf16), values[...]) + carried * jnp.exp((column_of(chunk) + 1.0) * decay)
    center = raw - jnp.mean(raw, axis=1, keepdims=True)
    variance = jnp.mean(center * center, axis=1, keepdims=True)
    gain = jnp.where(head == 0, gains[:, :value], gains[:, value:])
    ret = center * lax.rsqrt(variance + EPSILON) * gain
    joined = [ret * (1.0 / SMALL_WEIGHT), fox * (1.0 / FOX_OUT_WEIGHT)]
    mix[...] = jnp.concatenate(joined, axis=1).astype(bf16)


def output_kernel(mixes, weights, out, *, cores):
    parts = mixes.shape[0] // cores
    summed = jnp.zeros(out.shape, jnp.float32)
    for k in range(parts):
        partial = sum(
            dot(mixes[c * parts + k], weights[c * parts + k], NT) for c in range(cores)
        )
        summed = summed + partial.astype(jnp.bfloat16).astype(jnp.float32)
    out[...] = summed.astype(out.dtype)


def kernel(body, out_shape, in_specs, limit):
    return pl.pallas_call(
        body,
        out_shape=out_shape,
        in_specs=in_specs,
        out_specs=VMEM,
        compiler_params=pltpu.CompilerParams(vmem_limit_bytes=limit * MIB),
    )


def whole(*shape):
    return pl.BlockSpec(shape, lambda i: (0,) * len(shape))


def layer(
    tokens,
    norm_gain,
    ret_query_weight,
    ret_key_weight,
    ret_value_weight,
    fox_query_weight,
    fox_key_weight,
    fox_value_weight,
    ret_decay,
    ret_state,
    head_norm_gain,
    fox_gates,
    ret_out_weight,
    fox_out_weight,
):
    f32, bf16, f16 = jnp.float32, jnp.bfloat16, jnp.float16
    chip, core = lax.axis_index("sp_0"), lax.axis_index("sp_1")
    cores, tp = lax.axis_size("sp_1"), lax.axis_size("tp")
    rows, width = tokens.shape
    chunk = rows * cores
    key, value = ret_query_weight.shape[1] // cores, ret_value_weight.shape[1] // cores
    place = jnp.stack([chip, core]).astype(jnp.int32)

    peers = cores * tp
    shard = fox_key_weight.shape[0]
    lanes = 6 * value + 2 * key
    padded = lanes + -lanes % 128
    packed, sent = pl.pallas_call(
        pack_kernel,
        out_shape=(
            jax.ShapeDtypeStruct((cores, shard, padded), bf16),
            jax.ShapeDtypeStruct((peers, rows, width), bf16),
        ),
        grid=(1,),
        in_specs=[HBM]
        + [whole(shard, size * cores) for size in (value,) * 6 + (key,) * 2],
        out_specs=(whole(cores, shard, padded), HBM),
        scratch_shapes=[pltpu.SemaphoreType.DMA((peers,))],
        name="pack",
    )(
        tokens,
        ret_out_weight.T,
        fox_out_weight.T,
        fox_key_weight,
        fox_value_weight,
        fox_query_weight,
        ret_value_weight,
        ret_key_weight,
        ret_query_weight,
    )
    wide = lax.all_to_all(sent, CHIP, 0, 0, tiled=True)

    packed = lax.all_to_all(packed, "sp_1", 0, 0, tiled=True).reshape(-1, padded)
    widths = (value, value, value, value, value, value, key, key, padded - lanes)
    scales = (SMALL_WEIGHT, FOX_OUT_WEIGHT, SMALL_WEIGHT, SMALL_WEIGHT, QUERY_WEIGHT)
    scales += (SMALL_WEIGHT, SMALL_WEIGHT, SMALL_WEIGHT, 1.0)
    forth = jnp.concatenate([jnp.full((w,), s, f32) for w, s in zip(widths, scales)])
    weights = lax.all_gather(
        (packed.astype(f32) * forth).astype(f16), "sp_0", axis=0, tiled=True
    )
    weights = weights.astype(f32).astype(bf16)
    *parts, payload, sent = pl.pallas_call(
        lambda *refs: project_kernel(*refs, key=key, cores=cores),
        out_shape=(
            jax.ShapeDtypeStruct((chunk, 2 * value), bf16),
            jax.ShapeDtypeStruct((chunk, value), bf16),
            jax.ShapeDtypeStruct((chunk, key), bf16),
            jax.ShapeDtypeStruct((chunk, key), bf16),
            jax.ShapeDtypeStruct((chunk + key, 2 * value), f32),
            jax.ShapeDtypeStruct((peers, weights.shape[0], 2 * value), bf16),
        ),
        in_specs=[SMEM, SMEM, VMEM, VMEM, HBM, VMEM],
        out_specs=(VMEM,) * 5 + (HBM,),
        scratch_shapes=[
            pltpu.VMEM(weights.shape, bf16),
            pltpu.SemaphoreType.DMA,
            pltpu.SemaphoreType.DMA((peers,)),
        ],
        compiler_params=pltpu.CompilerParams(vmem_limit_bytes=20 * MIB),
        name="project",
    )(place, ret_decay, wide, norm_gain.reshape(tp, 1, width), weights, (1.0 / forth)[None])

    out_weights = lax.all_to_all(sent, CHIP, 0, 0, tiled=True)

    gathered = lax.all_gather(payload.astype(f16), "sp_0", axis=0, tiled=False)
    gathered = gathered.astype(f32).astype(bf16)

    mix = kernel(
        lambda *refs: mix_kernel(*refs, key=key),
        jax.ShapeDtypeStruct((chunk, 2 * value), bf16),
        [SMEM, SMEM] + [VMEM] * 8,
        24,
    )(
        place,
        ret_decay,
        *parts,
        gathered,
        fox_gates.T,
        ret_state,
        head_norm_gain[None],
    )

    final = rows // tp
    mixes = lax.all_to_all(mix.reshape(cores * tp, final, -1), CHIP, 0, 0, tiled=True)
    features = out_weights.shape[1]
    block = features // 4
    return pl.pallas_call(
        lambda *refs: output_kernel(*refs, cores=cores),
        out_shape=jax.ShapeDtypeStruct((final, features), bf16),
        grid=(features // block,),
        in_specs=[
            whole(*mixes.shape),
            pl.BlockSpec((peers, block, 2 * value), lambda i: (0, i, 0)),
        ],
        out_specs=pl.BlockSpec((final, block), lambda i: (0, i)),
        name="output",
    )(mixes, out_weights)


def solution(mesh):
    torus = Mesh(
        mesh.devices.reshape(mesh.shape["grp"], mesh.shape["sp"] // 2, 2, mesh.shape["tp"]),
        ("grp", "sp_0", "sp_1", "tp"),
    )
    return jax.shard_map(
        layer,
        mesh=torus,
        in_specs=(
            P(GRP_SP, "tp"),
            P(),
            P(SP, "tp"),
            P(SP, "tp"),
            P(SP, "tp"),
            P(SP, "tp"),
            P(SP, "tp"),
            P(SP, "tp"),
            P("tp"),
            P(("grp", "tp"), None, None),
            P("tp"),
            P("grp", "tp"),
            P("tp", SP),
            P("tp", SP),
        ),
        out_specs=P(GRP_SP_TP, None),
        check_vma=False,
    )
```

```python
import jax
import jax.numpy as jnp
from jax import lax
from jax.experimental import pallas as pl
from jax.experimental.pallas import tpu as pltpu
from jax.sharding import Mesh
from jax.sharding import PartitionSpec as P


SP = ("sp_0", "sp_1")
CHIP = ("sp_1", "tp")
GRP_SP = ("grp", "sp_0", "sp_1")
GRP_SP_TP = ("grp", "sp_0", "sp_1", "tp")

EPSILON = 1e-06
LOG2E = 1.4426950408889634
MIB = 2**20

SMALL_WEIGHT = 2.0**18
QUERY_WEIGHT = 2.0**12
FOX_OUT_WEIGHT = 2.0**15
KEY_VALUE = 2.0**7
STATE = 2.0**-9
STATE_LOW = 2.0**8

VMEM = pl.BlockSpec(memory_space=pltpu.VMEM)
SMEM = pl.BlockSpec(memory_space=pltpu.SMEM)
HBM = pl.BlockSpec(memory_space=pltpu.HBM)
NT = (((1,), (1,)), ((), ()))
TN = (((0,), (0,)), ((), ()))


def dot(a, b, dims=(((1,), (0,)), ((), ()))):
    return lax.dot_general(a, b, dims, preferred_element_type=jnp.float32)


def two_terms(x):
    high = x.astype(jnp.bfloat16)
    return high, (x - high.astype(jnp.float32)).astype(jnp.bfloat16)


def column_of(count):
    return lax.broadcasted_iota(jnp.int32, (count, 1), 0).astype(jnp.float32)


def copies(source, target, signals):
    return [
        pltpu.make_async_copy(source, target.at[k], signals.at[k]) for k in range(target.shape[0])
    ]


def pack_kernel(
    core, tokens, out_ret, out_fox, fk, fv, fq, rv, rk, rq, mine, theirs, sent, signals
):
    f32 = jnp.float32
    heads = 2
    started = copies(tokens, sent, signals)
    for copy in started:
        copy.start()

    def columns(ref, h):
        size = ref.shape[1] // heads
        return ref[...].astype(f32)[:, h * size : (h + 1) * size]

    both = []
    for h in range(heads):
        parts = [columns(ref, h) for ref in (out_ret, out_fox, fk, fv, fq, rv, rk, rq)]
        joined = jnp.concatenate(parts, axis=1)
        blank = mine.shape[1] - joined.shape[1]
        both.append(jnp.concatenate([joined, jnp.zeros((joined.shape[0], blank), f32)], axis=1))
    shard = both[0].shape[0]
    for c in range(heads):
        at = slice(c * shard, (c + 1) * shard)
        mine[at, :] = jnp.where(core[0] == c, both[c], 0.0).astype(mine.dtype)
        theirs[at, :] = jnp.where(core[0] == c, both[1 - c], 0.0).astype(theirs.dtype)
    for copy in started:
        copy.wait()


def project_kernel(
    place,
    decays,
    tokens,
    gains,
    weights,
    back,
    query,
    values,
    keys,
    queries,
    payload,
    *,
    key,
    cores,
):
    f32, bf16 = jnp.float32, jnp.bfloat16
    width = tokens.shape[1]
    parts, value = weights.shape[0], 2 * key
    rows = tokens.shape[0] // (cores * parts)
    first, last = 2 * value, 6 * value + 2 * key
    factors = []
    for c in range(cores):
        square = jnp.zeros((rows, 1), f32)
        for k in range(parts):
            x = tokens[(c * parts + k) * rows : (c * parts + k + 1) * rows, :].astype(f32)
            square = square + jnp.sum(x * x, axis=1, keepdims=True)
        factors.append(lax.rsqrt(square * (1.0 / (parts * width)) + EPSILON))
    for c in range(cores):
        total = jnp.zeros((rows, last - first), f32)
        for k in range(parts):
            x = tokens[(c * parts + k) * rows : (c * parts + k + 1) * rows, :].astype(f32)
            normed = (x * factors[c] * gains[k]).astype(bf16)
            total = total + dot(normed, weights[k][:, first:last])
        total = (total * back[:, first:last]).astype(bf16)
        at = slice(c * rows, (c + 1) * rows)
        payload[at, :] = total[:, : 2 * value].astype(f32) * KEY_VALUE
        lane = lax.broadcasted_iota(jnp.int32, (rows, 2 * value), 1)
        mixed = total[:, 2 * value : 4 * value].astype(f32)
        query[at, :] = jnp.where(lane < value, mixed, 0.0).astype(bf16)
        values[at, :] = total[:, 3 * value : 4 * value]
        keys[at, :] = total[:, 4 * value : 4 * value + key]
        queries[at, :] = total[:, 4 * value + key : 4 * value + 2 * key]
    chunk = rows * cores
    trailing = jnp.exp((chunk - 1.0 - column_of(chunk)) * decays[place[1]]) * key ** (-0.5)
    high, low = two_terms(keys[...].astype(f32) * trailing)
    summary = (dot(high, values[...], TN) + dot(low, values[...], TN)) * STATE
    high = summary.astype(bf16).astype(f32)
    payload[chunk:, :] = jnp.concatenate([high, (summary - high) * STATE_LOW], axis=1)


def mix_kernel(place, decays, query, values, keys, queries, gathered, gates, state, gains, mix, *, key):
    f32, bf16 = jnp.float32, jnp.bfloat16
    chunk, value = query.shape[0], 2 * key
    own, head = place[0], place[1]
    decay = decays[head]
    attending = query[...]
    scale = value ** (-0.5) * LOG2E / KEY_VALUE

    def gates_of(j):
        pair = gates[:, pl.ds(pl.multiple_of(j * chunk, chunk), chunk)]
        return jnp.where(head == 0, pair[:1], pair[1:])

    base = jnp.max(gates_of(own), axis=1, keepdims=True)

    def logits_of(j):
        pairs = gathered[j, :chunk, :]
        return dot(attending, pairs, NT) * scale - (gates_of(j) - base) * LOG2E, pairs

    row = lax.broadcasted_iota(jnp.int32, (chunk, chunk), 0)
    col = lax.broadcasted_iota(jnp.int32, (chunk, chunk), 1)
    t, pairs = logits_of(own)
    t = jnp.where(col <= row, t, -jnp.inf)
    top = jnp.max(t, axis=1, keepdims=True)
    p = jnp.exp2(t - top)
    total = jnp.sum(p, axis=1, keepdims=True)
    mixed = dot(p.astype(bf16), pairs)

    ones = jnp.ones((1, 2 * value), f32)
    per_chunk = jnp.exp(ones * (chunk * decay))

    def step(j, carry):
        top, total, mixed, memory = carry
        t, pairs = logits_of(j)
        new = jnp.maximum(top, jnp.max(t, axis=1, keepdims=True))
        p = jnp.exp2(t - new)
        keep = jnp.exp2(top - new)
        total = total * keep + jnp.sum(p, axis=1, keepdims=True)
        mixed = mixed * keep + dot(p.astype(bf16), pairs)
        memory = memory * per_chunk + gathered[j, chunk:, :].astype(f32)
        return new, total, mixed, memory

    memory = jnp.zeros((key, 2 * value), f32)
    _, total, mixed, memory = lax.fori_loop(0, own, step, (top, total, mixed, memory))
    fox = (mixed * (1.0 / KEY_VALUE) / total)[:, value:]

    memory = (memory[:, :value] + memory[:, value:] * (1.0 / STATE_LOW)) * (1.0 / STATE)
    first = (own * chunk).astype(f32)
    entering = jnp.exp(ones[:, :value] * (first * decay)) * state[head] + memory
    ret_query = queries[...]
    spread = (row - col).astype(f32)
    within = jnp.where(col <= row, jnp.exp(jnp.maximum(spread, 0.0) * decay), 0.0)
    near = dot(ret_query, keys[...], NT) * within * key ** (-0.5)
    high, low = two_terms(entering)
    carried = dot(ret_query, high) + dot(ret_query, low)
    raw = dot(near.astype(bf16), values[...]) + carried * jnp.exp((column_of(chunk) + 1.0) * decay)
    center = raw - jnp.mean(raw, axis=1, keepdims=True)
    variance = jnp.mean(center * center, axis=1, keepdims=True)
    gain = jnp.where(head == 0, gains[:, :value], gains[:, value:])
    ret = center * lax.rsqrt(variance + EPSILON) * gain
    joined = [ret * (1.0 / SMALL_WEIGHT), fox * (1.0 / FOX_OUT_WEIGHT)]
    mix[...] = jnp.concatenate(joined, axis=1).astype(bf16)


def output_kernel(mixes, weights, out, *, cores):
    parts = mixes.shape[0] // cores
    summed = jnp.zeros(out.shape, jnp.float32)
    for k in range(parts):
        partial = sum(
            dot(mixes[c * parts + k], weights[c * parts + k], NT) for c in range(cores)
        )
        summed = summed + partial.astype(jnp.bfloat16).astype(jnp.float32)
    out[...] = summed.astype(out.dtype)


def kernel(body, out_shape, in_specs, limit):
    return pl.pallas_call(
        body,
        out_shape=out_shape,
        in_specs=in_specs,
        out_specs=VMEM,
        compiler_params=pltpu.CompilerParams(vmem_limit_bytes=limit * MIB),
    )


def whole(*shape):
    return pl.BlockSpec(shape, lambda i: (0,) * len(shape))


def layer(
    tokens,
    norm_gain,
    ret_query_weight,
    ret_key_weight,
    ret_value_weight,
    fox_query_weight,
    fox_key_weight,
    fox_value_weight,
    ret_decay,
    ret_state,
    head_norm_gain,
    fox_gates,
    ret_out_weight,
    fox_out_weight,
):
    f32, bf16, f16 = jnp.float32, jnp.bfloat16, jnp.float16
    chip, core = lax.axis_index("sp_0"), lax.axis_index("sp_1")
    cores, tp = lax.axis_size("sp_1"), lax.axis_size("tp")
    rows, width = tokens.shape
    chunk = rows * cores
    key, value = ret_query_weight.shape[1] // cores, ret_value_weight.shape[1] // cores
    place = jnp.stack([chip, core]).astype(jnp.int32)

    peers = cores * tp
    shard = fox_key_weight.shape[0]
    chip_shard = shard * cores
    lanes = 6 * value + 2 * key
    padded = lanes + -lanes % 128
    mine, theirs, sent = pl.pallas_call(
        pack_kernel,
        out_shape=(
            jax.ShapeDtypeStruct((chip_shard, padded), bf16),
            jax.ShapeDtypeStruct((chip_shard, padded), bf16),
            jax.ShapeDtypeStruct((peers, rows, width), bf16),
        ),
        grid=(1,),
        in_specs=[SMEM, whole(rows, width)]
        + [whole(shard, size * cores) for size in (value,) * 6 + (key,) * 2],
        out_specs=(VMEM, VMEM, HBM),
        scratch_shapes=[pltpu.SemaphoreType.DMA((peers,))],
        name="pack",
    )(
        place[1:],
        tokens,
        ret_out_weight.T,
        fox_out_weight.T,
        fox_key_weight,
        fox_value_weight,
        fox_query_weight,
        ret_value_weight,
        ret_key_weight,
        ret_query_weight,
    )
    wide = lax.all_to_all(sent, CHIP, 0, 0, tiled=True)

    got = lax.ppermute(theirs, "sp_1", [(0, 1), (1, 0)])
    packed = mine.astype(f32) + got.astype(f32)
    widths = (value, value, value, value, value, value, key, key, padded - lanes)
    scales = (SMALL_WEIGHT, FOX_OUT_WEIGHT, SMALL_WEIGHT, SMALL_WEIGHT, QUERY_WEIGHT)
    scales += (SMALL_WEIGHT, SMALL_WEIGHT, SMALL_WEIGHT, 1.0)
    forth = jnp.concatenate([jnp.full((w,), s, f32) for w, s in zip(widths, scales)])
    weights = lax.all_gather(
        (packed * forth).astype(f16), "sp_0", axis=0, tiled=True
    )
    weights = weights.astype(f32).astype(bf16)
    *parts, payload = pl.pallas_call(
        lambda *refs: project_kernel(*refs, key=key, cores=cores),
        out_shape=(
            jax.ShapeDtypeStruct((chunk, 2 * value), bf16),
            jax.ShapeDtypeStruct((chunk, value), bf16),
            jax.ShapeDtypeStruct((chunk, key), bf16),
            jax.ShapeDtypeStruct((chunk, key), bf16),
            jax.ShapeDtypeStruct((chunk + key, 2 * value), f32),
        ),
        in_specs=[SMEM, SMEM] + [VMEM] * 4,
        out_specs=(VMEM,) * 5,
        compiler_params=pltpu.CompilerParams(vmem_limit_bytes=20 * MIB),
        name="project",
    )(
        place,
        ret_decay,
        wide.reshape(-1, width),
        norm_gain.reshape(tp, 1, width),
        weights.reshape(tp, width, padded),
        (1.0 / forth)[None],
    )

    sent = jnp.broadcast_to(weights[None, :, : 2 * value], (peers, weights.shape[0], 2 * value))
    out_weights = lax.all_to_all(sent, CHIP, 0, 0, tiled=True)

    gathered = lax.all_gather(payload.astype(f16), "sp_0", axis=0, tiled=False)
    gathered = gathered.astype(f32).astype(bf16)

    mix = kernel(
        lambda *refs: mix_kernel(*refs, key=key),
        jax.ShapeDtypeStruct((chunk, 2 * value), bf16),
        [SMEM, SMEM] + [VMEM] * 8,
        24,
    )(
        place,
        ret_decay,
        *parts,
        gathered,
        fox_gates.T,
        ret_state,
        head_norm_gain[None],
    )

    final = rows // tp
    mixes = lax.all_to_all(mix.reshape(cores * tp, final, -1), CHIP, 0, 0, tiled=True)
    return kernel(
        lambda *refs: output_kernel(*refs, cores=cores),
        jax.ShapeDtypeStruct((final, out_weights.shape[1]), bf16),
        [VMEM, VMEM],
        16,
    )(mixes, out_weights)


def solution(mesh):
    torus = Mesh(
        mesh.devices.reshape(mesh.shape["grp"], mesh.shape["sp"] // 2, 2, mesh.shape["tp"]),
        ("grp", "sp_0", "sp_1", "tp"),
    )
    return jax.shard_map(
        layer,
        mesh=torus,
        in_specs=(
            P(GRP_SP, "tp"),
            P(),
            P(SP, "tp"),
            P(SP, "tp"),
            P(SP, "tp"),
            P(SP, "tp"),
            P(SP, "tp"),
            P(SP, "tp"),
            P("tp"),
            P(("grp", "tp"), None, None),
            P("tp"),
            P("grp", "tp"),
            P("tp", SP),
            P("tp", SP),
        ),
        out_specs=P(GRP_SP_TP, None),
        check_vma=False,
    )
```

```python
import jax
import jax.numpy as jnp
from jax import lax
from jax.experimental import pallas as pl
from jax.experimental.pallas import tpu as pltpu
from jax.sharding import Mesh
from jax.sharding import PartitionSpec as P


SP = ("sp_0", "sp_1")
CHIP = ("sp_1", "tp")
GRP_SP = ("grp", "sp_0", "sp_1")
GRP_SP_TP = ("grp", "sp_0", "sp_1", "tp")

EPSILON = 1e-06
LOG2E = 1.4426950408889634
MIB = 2**20

SMALL_WEIGHT = 2.0**18
QUERY_WEIGHT = 2.0**12
FOX_OUT_WEIGHT = 2.0**15
KEY_VALUE = 2.0**7
STATE = 2.0**-9
STATE_LOW = 2.0**8

VMEM = pl.BlockSpec(memory_space=pltpu.VMEM)
SMEM = pl.BlockSpec(memory_space=pltpu.SMEM)
HBM = pl.BlockSpec(memory_space=pltpu.HBM)
NT = (((1,), (1,)), ((), ()))
TN = (((0,), (0,)), ((), ()))


def dot(a, b, dims=(((1,), (0,)), ((), ()))):
    return lax.dot_general(a, b, dims, preferred_element_type=jnp.float32)


def two_terms(x):
    high = x.astype(jnp.bfloat16)
    return high, (x - high.astype(jnp.float32)).astype(jnp.bfloat16)


def column_of(count):
    return lax.broadcasted_iota(jnp.int32, (count, 1), 0).astype(jnp.float32)


def copies(source, target, signals):
    return [
        pltpu.make_async_copy(source, target.at[k], signals.at[k]) for k in range(target.shape[0])
    ]


def arrivals(source, target, signals):
    return [
        pltpu.make_async_copy(source.at[k], target.at[k], signals.at[k])
        for k in range(target.shape[0])
    ]


def pack_kernel(
    core, tokens, out_ret, out_fox, fk, fv, fq, rv, rk, rq, mine, theirs, sent, signals
):
    f32 = jnp.float32
    heads = 2
    started = copies(tokens, sent, signals)
    for copy in started:
        copy.start()

    def columns(ref, h):
        size = ref.shape[1] // heads
        return ref[...].astype(f32)[:, h * size : (h + 1) * size]

    both = []
    for h in range(heads):
        parts = [columns(ref, h) for ref in (out_ret, out_fox, fk, fv, fq, rv, rk, rq)]
        joined = jnp.concatenate(parts, axis=1)
        blank = mine.shape[1] - joined.shape[1]
        both.append(jnp.concatenate([joined, jnp.zeros((joined.shape[0], blank), f32)], axis=1))
    shard = both[0].shape[0]
    for c in range(heads):
        at = slice(c * shard, (c + 1) * shard)
        mine[at, :] = jnp.where(core[0] == c, both[c], 0.0).astype(mine.dtype)
        theirs[at, :] = jnp.where(core[0] == c, both[1 - c], 0.0).astype(theirs.dtype)
    for copy in started:
        copy.wait()


def project_kernel(
    place,
    decays,
    arrived,
    gains,
    weights,
    back,
    query,
    values,
    keys,
    queries,
    payload,
    tokens,
    signals,
    *,
    key,
    cores,
):
    f32, bf16 = jnp.float32, jnp.bfloat16
    rows, width = tokens.shape[1:]
    parts, value = weights.shape[0], 2 * key
    arriving = arrivals(arrived, tokens, signals)
    for copy in arriving:
        copy.start()
    first, last = 2 * value, 6 * value + 2 * key
    factors = []
    for c in range(cores):
        square = jnp.zeros((rows, 1), f32)
        for k in range(parts):
            arriving[c * parts + k].wait()
            x = tokens[c * parts + k].astype(f32)
            square = square + jnp.sum(x * x, axis=1, keepdims=True)
        factors.append(lax.rsqrt(square * (1.0 / (parts * width)) + EPSILON))
    for c in range(cores):
        total = jnp.zeros((rows, last - first), f32)
        for k in range(parts):
            x = tokens[c * parts + k].astype(f32)
            normed = (x * factors[c] * gains[k]).astype(bf16)
            total = total + dot(normed, weights[k][:, first:last])
        total = (total * back[:, first:last]).astype(bf16)
        at = slice(c * rows, (c + 1) * rows)
        payload[at, :] = total[:, : 2 * value].astype(f32) * KEY_VALUE
        lane = lax.broadcasted_iota(jnp.int32, (rows, 2 * value), 1)
        mixed = total[:, 2 * value : 4 * value].astype(f32)
        query[at, :] = jnp.where(lane < value, mixed, 0.0).astype(bf16)
        values[at, :] = total[:, 3 * value : 4 * value]
        keys[at, :] = total[:, 4 * value : 4 * value + key]
        queries[at, :] = total[:, 4 * value + key : 4 * value + 2 * key]
    chunk = rows * cores
    trailing = jnp.exp((chunk - 1.0 - column_of(chunk)) * decays[place[1]]) * key ** (-0.5)
    high, low = two_terms(keys[...].astype(f32) * trailing)
    summary = (dot(high, values[...], TN) + dot(low, values[...], TN)) * STATE
    high = summary.astype(bf16).astype(f32)
    payload[chunk:, :] = jnp.concatenate([high, (summary - high) * STATE_LOW], axis=1)


def mix_kernel(place, decays, query, values, keys, queries, gathered, gates, state, gains, mix, *, key):
    f32, bf16 = jnp.float32, jnp.bfloat16
    chunk, value = query.shape[0], 2 * key
    own, head = place[0], place[1]
    decay = decays[head]
    attending = query[...]
    scale = value ** (-0.5) * LOG2E / KEY_VALUE

    def gates_of(j):
        pair = gates[:, pl.ds(pl.multiple_of(j * chunk, chunk), chunk)]
        return jnp.where(head == 0, pair[:1], pair[1:])

    base = jnp.max(gates_of(own), axis=1, keepdims=True)

    def logits_of(j):
        pairs = gathered[j, :chunk, :]
        return dot(attending, pairs, NT) * scale - (gates_of(j) - base) * LOG2E, pairs

    row = lax.broadcasted_iota(jnp.int32, (chunk, chunk), 0)
    col = lax.broadcasted_iota(jnp.int32, (chunk, chunk), 1)
    t, pairs = logits_of(own)
    t = jnp.where(col <= row, t, -jnp.inf)
    top = jnp.max(t, axis=1, keepdims=True)
    p = jnp.exp2(t - top)
    total = jnp.sum(p, axis=1, keepdims=True)
    mixed = dot(p.astype(bf16), pairs)

    ones = jnp.ones((1, 2 * value), f32)
    per_chunk = jnp.exp(ones * (chunk * decay))

    def step(j, carry):
        top, total, mixed, memory = carry
        t, pairs = logits_of(j)
        new = jnp.maximum(top, jnp.max(t, axis=1, keepdims=True))
        p = jnp.exp2(t - new)
        keep = jnp.exp2(top - new)
        total = total * keep + jnp.sum(p, axis=1, keepdims=True)
        mixed = mixed * keep + dot(p.astype(bf16), pairs)
        memory = memory * per_chunk + gathered[j, chunk:, :].astype(f32)
        return new, total, mixed, memory

    memory = jnp.zeros((key, 2 * value), f32)
    _, total, mixed, memory = lax.fori_loop(0, own, step, (top, total, mixed, memory))
    fox = (mixed * (1.0 / KEY_VALUE) / total)[:, value:]

    memory = (memory[:, :value] + memory[:, value:] * (1.0 / STATE_LOW)) * (1.0 / STATE)
    first = (own * chunk).astype(f32)
    entering = jnp.exp(ones[:, :value] * (first * decay)) * state[head] + memory
    ret_query = queries[...]
    spread = (row - col).astype(f32)
    within = jnp.where(col <= row, jnp.exp(jnp.maximum(spread, 0.0) * decay), 0.0)
    near = dot(ret_query, keys[...], NT) * within * key ** (-0.5)
    high, low = two_terms(entering)
    carried = dot(ret_query, high) + dot(ret_query, low)
    raw = dot(near.astype(bf16), values[...]) + carried * jnp.exp((column_of(chunk) + 1.0) * decay)
    center = raw - jnp.mean(raw, axis=1, keepdims=True)
    variance = jnp.mean(center * center, axis=1, keepdims=True)
    gain = jnp.where(head == 0, gains[:, :value], gains[:, value:])
    ret = center * lax.rsqrt(variance + EPSILON) * gain
    joined = [ret * (1.0 / SMALL_WEIGHT), fox * (1.0 / FOX_OUT_WEIGHT)]
    mix[...] = jnp.concatenate(joined, axis=1).astype(bf16)


def output_kernel(mixes, stored, out, weights, signals, *, cores):
    parts = mixes.shape[0] // cores
    arriving = arrivals(stored, weights, signals)
    for k in range(parts):
        for c in range(cores):
            arriving[c * parts + k].start()
    summed = jnp.zeros(out.shape, jnp.float32)
    for k in range(parts):
        for c in range(cores):
            arriving[c * parts + k].wait()
        partial = sum(
            dot(mixes[c * parts + k], weights[c * parts + k], NT) for c in range(cores)
        )
        summed = summed + partial.astype(jnp.bfloat16).astype(jnp.float32)
    out[...] = summed.astype(out.dtype)


def kernel(body, out_shape, in_specs, limit):
    return pl.pallas_call(
        body,
        out_shape=out_shape,
        in_specs=in_specs,
        out_specs=VMEM,
        compiler_params=pltpu.CompilerParams(vmem_limit_bytes=limit * MIB),
    )


def whole(*shape):
    return pl.BlockSpec(shape, lambda i: (0,) * len(shape))


def layer(
    tokens,
    norm_gain,
    ret_query_weight,
    ret_key_weight,
    ret_value_weight,
    fox_query_weight,
    fox_key_weight,
    fox_value_weight,
    ret_decay,
    ret_state,
    head_norm_gain,
    fox_gates,
    ret_out_weight,
    fox_out_weight,
):
    f32, bf16, f16 = jnp.float32, jnp.bfloat16, jnp.float16
    chip, core = lax.axis_index("sp_0"), lax.axis_index("sp_1")
    cores, tp = lax.axis_size("sp_1"), lax.axis_size("tp")
    rows, width = tokens.shape
    chunk = rows * cores
    key, value = ret_query_weight.shape[1] // cores, ret_value_weight.shape[1] // cores
    place = jnp.stack([chip, core]).astype(jnp.int32)

    peers = cores * tp
    shard = fox_key_weight.shape[0]
    chip_shard = shard * cores
    lanes = 6 * value + 2 * key
    padded = lanes + -lanes % 128
    mine, theirs, sent = pl.pallas_call(
        pack_kernel,
        out_shape=(
            jax.ShapeDtypeStruct((chip_shard, padded), bf16),
            jax.ShapeDtypeStruct((chip_shard, padded), bf16),
            jax.ShapeDtypeStruct((peers, rows, width), bf16),
        ),
        grid=(1,),
        in_specs=[SMEM, whole(rows, width)]
        + [whole(shard, size * cores) for size in (value,) * 6 + (key,) * 2],
        out_specs=(VMEM, VMEM, HBM),
        scratch_shapes=[pltpu.SemaphoreType.DMA((peers,))],
        name="pack",
    )(
        place[1:],
        tokens,
        ret_out_weight.T,
        fox_out_weight.T,
        fox_key_weight,
        fox_value_weight,
        fox_query_weight,
        ret_value_weight,
        ret_key_weight,
        ret_query_weight,
    )
    wide = lax.all_to_all(sent, CHIP, 0, 0, tiled=True)

    got = lax.ppermute(theirs, "sp_1", [(0, 1), (1, 0)])
    packed = mine.astype(f32) + got.astype(f32)
    widths = (value, value, value, value, value, value, key, key, padded - lanes)
    scales = (SMALL_WEIGHT, FOX_OUT_WEIGHT, SMALL_WEIGHT, SMALL_WEIGHT, QUERY_WEIGHT)
    scales += (SMALL_WEIGHT, SMALL_WEIGHT, SMALL_WEIGHT, 1.0)
    forth = jnp.concatenate([jnp.full((w,), s, f32) for w, s in zip(widths, scales)])
    weights = lax.all_gather(
        (packed * forth).astype(f16), "sp_0", axis=0, tiled=True
    )
    weights = weights.astype(f32).astype(bf16)
    *parts, payload = pl.pallas_call(
        lambda *refs: project_kernel(*refs, key=key, cores=cores),
        out_shape=(
            jax.ShapeDtypeStruct((chunk, 2 * value), bf16),
            jax.ShapeDtypeStruct((chunk, value), bf16),
            jax.ShapeDtypeStruct((chunk, key), bf16),
            jax.ShapeDtypeStruct((chunk, key), bf16),
            jax.ShapeDtypeStruct((chunk + key, 2 * value), f32),
        ),
        in_specs=[SMEM, SMEM, HBM, VMEM, VMEM, VMEM],
        out_specs=(VMEM,) * 5,
        scratch_shapes=[
            pltpu.VMEM(wide.shape, bf16),
            pltpu.SemaphoreType.DMA((peers,)),
        ],
        compiler_params=pltpu.CompilerParams(vmem_limit_bytes=20 * MIB),
        name="project",
    )(
        place,
        ret_decay,
        wide,
        norm_gain.reshape(tp, 1, width),
        weights.reshape(tp, width, padded),
        (1.0 / forth)[None],
    )

    sent = jnp.broadcast_to(weights[None, :, : 2 * value], (peers, weights.shape[0], 2 * value))
    out_weights = lax.all_to_all(sent, CHIP, 0, 0, tiled=True)

    gathered = lax.all_gather(payload.astype(f16), "sp_0", axis=0, tiled=False)
    gathered = gathered.astype(f32).astype(bf16)

    mix = kernel(
        lambda *refs: mix_kernel(*refs, key=key),
        jax.ShapeDtypeStruct((chunk, 2 * value), bf16),
        [SMEM, SMEM] + [VMEM] * 8,
        24,
    )(
        place,
        ret_decay,
        *parts,
        gathered,
        fox_gates.T,
        ret_state,
        head_norm_gain[None],
    )

    final = rows // tp
    mixes = lax.all_to_all(mix.reshape(cores * tp, final, -1), CHIP, 0, 0, tiled=True)
    return pl.pallas_call(
        lambda *refs: output_kernel(*refs, cores=cores),
        out_shape=jax.ShapeDtypeStruct((final, out_weights.shape[1]), bf16),
        in_specs=[VMEM, HBM],
        out_specs=VMEM,
        scratch_shapes=[
            pltpu.VMEM(out_weights.shape, bf16),
            pltpu.SemaphoreType.DMA((peers,)),
        ],
        compiler_params=pltpu.CompilerParams(vmem_limit_bytes=16 * MIB),
        name="output",
    )(mixes, out_weights)


def solution(mesh):
    torus = Mesh(
        mesh.devices.reshape(mesh.shape["grp"], mesh.shape["sp"] // 2, 2, mesh.shape["tp"]),
        ("grp", "sp_0", "sp_1", "tp"),
    )
    return jax.shard_map(
        layer,
        mesh=torus,
        in_specs=(
            P(GRP_SP, "tp"),
            P(),
            P(SP, "tp"),
            P(SP, "tp"),
            P(SP, "tp"),
            P(SP, "tp"),
            P(SP, "tp"),
            P(SP, "tp"),
            P("tp"),
            P(("grp", "tp"), None, None),
            P("tp"),
            P("grp", "tp"),
            P("tp", SP),
            P("tp", SP),
        ),
        out_specs=P(GRP_SP_TP, None),
        check_vma=False,
    )
```

```python
import jax
import jax.numpy as jnp
from jax import lax
from jax.experimental import pallas as pl
from jax.experimental.pallas import tpu as pltpu
from jax.sharding import Mesh
from jax.sharding import PartitionSpec as P


SP = ("sp_0", "sp_1")
CHIP = ("sp_1", "tp")
GRP_SP = ("grp", "sp_0", "sp_1")
GRP_SP_TP = ("grp", "sp_0", "sp_1", "tp")

EPSILON = 1e-06
LOG2E = 1.4426950408889634
MIB = 2**20

SMALL_WEIGHT = 2.0**18
QUERY_WEIGHT = 2.0**12
FOX_OUT_WEIGHT = 2.0**15
KEY_VALUE = 2.0**7
STATE = 2.0**-9
STATE_LOW = 2.0**8

VMEM = pl.BlockSpec(memory_space=pltpu.VMEM)
SMEM = pl.BlockSpec(memory_space=pltpu.SMEM)
HBM = pl.BlockSpec(memory_space=pltpu.HBM)
NT = (((1,), (1,)), ((), ()))
TN = (((0,), (0,)), ((), ()))


def dot(a, b, dims=(((1,), (0,)), ((), ()))):
    return lax.dot_general(a, b, dims, preferred_element_type=jnp.float32)


def two_terms(x):
    high = x.astype(jnp.bfloat16)
    return high, (x - high.astype(jnp.float32)).astype(jnp.bfloat16)


def column_of(count):
    return lax.broadcasted_iota(jnp.int32, (count, 1), 0).astype(jnp.float32)


def copies(source, target, signals):
    return [
        pltpu.make_async_copy(source, target.at[k], signals.at[k]) for k in range(target.shape[0])
    ]


def arrivals(source, target, signals):
    return [
        pltpu.make_async_copy(source.at[k], target.at[k], signals.at[k])
        for k in range(target.shape[0])
    ]


def pack_kernel(
    core, tokens, out_ret, out_fox, fk, fv, fq, rv, rk, rq, mine, theirs, sent, signals
):
    f32 = jnp.float32
    heads = 2
    started = copies(tokens, sent, signals)
    for copy in started:
        copy.start()

    def columns(ref, h, scale):
        size = ref.shape[1] // heads
        return ref[...].astype(f32)[:, h * size : (h + 1) * size] * scale

    groups = (
        ((out_ret, SMALL_WEIGHT), (out_fox, FOX_OUT_WEIGHT)),
        ((fk, SMALL_WEIGHT), (fv, SMALL_WEIGHT)),
        ((fq, QUERY_WEIGHT), (rv, SMALL_WEIGHT)),
        ((rk, SMALL_WEIGHT), (rq, SMALL_WEIGHT)),
    )
    both = [
        [jnp.concatenate([columns(ref, h, scale) for ref, scale in group], axis=1) for group in groups]
        for h in range(heads)
    ]
    first = core[0] == 0
    shard = both[0][0].shape[0]
    for c in range(heads):
        for g in range(3):
            at = slice((g * heads + c) * shard, (g * heads + c + 1) * shard)
            mine[at, :] = jnp.where(core[0] == c, both[c][g], 0.0).astype(mine.dtype)
            theirs[at, :] = jnp.where(core[0] == c, both[1 - c][g], 0.0).astype(theirs.dtype)
    at = slice(3 * heads * shard, (3 * heads + 1) * shard)

    def halves(left, right):
        left, right = jnp.where(first, left, 0.0), jnp.where(first, 0.0, right)
        return jnp.concatenate([left, right], axis=1)

    mine[at, :] = halves(both[0][3], both[1][3]).astype(mine.dtype)
    theirs[at, :] = halves(both[1][3], both[0][3]).astype(theirs.dtype)
    for copy in started:
        copy.wait()


def project_kernel(
    place,
    decays,
    tokens,
    gains,
    weights,
    query,
    values,
    keys,
    queries,
    payload,
    *,
    key,
    cores,
):
    f32, bf16 = jnp.float32, jnp.bfloat16
    width = tokens.shape[1]
    parts, value = gains.shape[0], 2 * key
    rows = tokens.shape[0] // (cores * parts)
    per = weights.shape[0] // parts
    side = width // per
    blocks = []
    for k in range(parts):
        at = slice(k * per, (k + 1) * per)
        pair = weights[at, side : 2 * side, :].reshape(width, 2 * value)
        mixed = weights[at, 2 * side : 3 * side, :].reshape(width, 2 * value)
        last = weights[at, 3 * side :, :]
        last = jnp.concatenate([last[:, :, :value], last[:, :, value:]], axis=1)
        blocks.append((pair, mixed, last.reshape(width, value)))
    factors = []
    for c in range(cores):
        square = jnp.zeros((rows, 1), f32)
        for k in range(parts):
            x = tokens[(c * parts + k) * rows : (c * parts + k + 1) * rows, :].astype(f32)
            square = square + jnp.sum(x * x, axis=1, keepdims=True)
        factors.append(lax.rsqrt(square * (1.0 / (parts * width)) + EPSILON))
    for c in range(cores):
        sums = [jnp.zeros((rows, block.shape[1]), f32) for block in blocks[0]]
        for k in range(parts):
            x = tokens[(c * parts + k) * rows : (c * parts + k + 1) * rows, :].astype(f32)
            normed = (x * factors[c] * gains[k]).astype(bf16)
            sums = [total + dot(normed, block) for total, block in zip(sums, blocks[k])]
        pair, mixed, last = sums
        lane = lax.broadcasted_iota(jnp.int32, (rows, 2 * value), 1)
        back = jnp.where(lane < value, 1.0 / QUERY_WEIGHT, 1.0 / SMALL_WEIGHT)
        pair = (pair * (1.0 / SMALL_WEIGHT)).astype(bf16)
        mixed = (mixed * back).astype(bf16)
        last = (last * (1.0 / SMALL_WEIGHT)).astype(bf16)
        at = slice(c * rows, (c + 1) * rows)
        payload[at, :] = pair.astype(f32) * KEY_VALUE
        query[at, :] = jnp.where(lane < value, mixed.astype(f32), 0.0).astype(bf16)
        values[at, :] = mixed[:, value:]
        keys[at, :] = last[:, :key]
        queries[at, :] = last[:, key:]
    chunk = rows * cores
    trailing = jnp.exp((chunk - 1.0 - column_of(chunk)) * decays[place[1]]) * key ** (-0.5)
    high, low = two_terms(keys[...].astype(f32) * trailing)
    summary = (dot(high, values[...], TN) + dot(low, values[...], TN)) * STATE
    high = summary.astype(bf16).astype(f32)
    payload[chunk:, :] = jnp.concatenate([high, (summary - high) * STATE_LOW], axis=1)


def mix_kernel(place, decays, query, values, keys, queries, gathered, gates, state, gains, mix, *, key):
    f32, bf16 = jnp.float32, jnp.bfloat16
    chunk, value = query.shape[0], 2 * key
    own, head = place[0], place[1]
    decay = decays[head]
    attending = query[...]
    scale = value ** (-0.5) * LOG2E / KEY_VALUE

    def gates_of(j):
        pair = gates[:, pl.ds(pl.multiple_of(j * chunk, chunk), chunk)]
        return jnp.where(head == 0, pair[:1], pair[1:])

    base = jnp.max(gates_of(own), axis=1, keepdims=True)

    def logits_of(j):
        pairs = gathered[j, :chunk, :]
        return dot(attending, pairs, NT) * scale - (gates_of(j) - base) * LOG2E, pairs

    row = lax.broadcasted_iota(jnp.int32, (chunk, chunk), 0)
    col = lax.broadcasted_iota(jnp.int32, (chunk, chunk), 1)
    t, pairs = logits_of(own)
    t = jnp.where(col <= row, t, -jnp.inf)
    top = jnp.max(t, axis=1, keepdims=True)
    p = jnp.exp2(t - top)
    total = jnp.sum(p, axis=1, keepdims=True)
    mixed = dot(p.astype(bf16), pairs)

    ones = jnp.ones((1, 2 * value), f32)
    per_chunk = jnp.exp(ones * (chunk * decay))

    def step(j, carry):
        top, total, mixed, memory = carry
        t, pairs = logits_of(j)
        new = jnp.maximum(top, jnp.max(t, axis=1, keepdims=True))
        p = jnp.exp2(t - new)
        keep = jnp.exp2(top - new)
        total = total * keep + jnp.sum(p, axis=1, keepdims=True)
        mixed = mixed * keep + dot(p.astype(bf16), pairs)
        memory = memory * per_chunk + gathered[j, chunk:, :].astype(f32)
        return new, total, mixed, memory

    memory = jnp.zeros((key, 2 * value), f32)
    _, total, mixed, memory = lax.fori_loop(0, own, step, (top, total, mixed, memory))
    fox = (mixed * (1.0 / KEY_VALUE) / total)[:, value:]

    memory = (memory[:, :value] + memory[:, value:] * (1.0 / STATE_LOW)) * (1.0 / STATE)
    first = (own * chunk).astype(f32)
    entering = jnp.exp(ones[:, :value] * (first * decay)) * state[head] + memory
    ret_query = queries[...]
    spread = (row - col).astype(f32)
    within = jnp.where(col <= row, jnp.exp(jnp.maximum(spread, 0.0) * decay), 0.0)
    near = dot(ret_query, keys[...], NT) * within * key ** (-0.5)
    high, low = two_terms(entering)
    carried = dot(ret_query, high) + dot(ret_query, low)
    raw = dot(near.astype(bf16), values[...]) + carried * jnp.exp((column_of(chunk) + 1.0) * decay)
    center = raw - jnp.mean(raw, axis=1, keepdims=True)
    variance = jnp.mean(center * center, axis=1, keepdims=True)
    gain = jnp.where(head == 0, gains[:, :value], gains[:, value:])
    ret = center * lax.rsqrt(variance + EPSILON) * gain
    joined = [ret * (1.0 / SMALL_WEIGHT), fox * (1.0 / FOX_OUT_WEIGHT)]
    mix[...] = jnp.concatenate(joined, axis=1).astype(bf16)


def output_kernel(mixes, stored, out, weights, signals, *, cores):
    parts = mixes.shape[0] // cores
    arriving = arrivals(stored, weights, signals)
    for k in range(parts):
        for c in range(cores):
            arriving[c * parts + k].start()
    summed = jnp.zeros(out.shape, jnp.float32)
    for k in range(parts):
        for c in range(cores):
            arriving[c * parts + k].wait()
        partial = sum(
            dot(mixes[c * parts + k], weights[c * parts + k], NT) for c in range(cores)
        )
        summed = summed + partial.astype(jnp.bfloat16).astype(jnp.float32)
    out[...] = summed.astype(out.dtype)


def kernel(body, out_shape, in_specs, limit):
    return pl.pallas_call(
        body,
        out_shape=out_shape,
        in_specs=in_specs,
        out_specs=VMEM,
        compiler_params=pltpu.CompilerParams(vmem_limit_bytes=limit * MIB),
    )


def whole(*shape):
    return pl.BlockSpec(shape, lambda i: (0,) * len(shape))


def layer(
    tokens,
    norm_gain,
    ret_query_weight,
    ret_key_weight,
    ret_value_weight,
    fox_query_weight,
    fox_key_weight,
    fox_value_weight,
    ret_decay,
    ret_state,
    head_norm_gain,
    fox_gates,
    ret_out_weight,
    fox_out_weight,
):
    f32, bf16, f16 = jnp.float32, jnp.bfloat16, jnp.float16
    chip, core = lax.axis_index("sp_0"), lax.axis_index("sp_1")
    cores, tp = lax.axis_size("sp_1"), lax.axis_size("tp")
    rows, width = tokens.shape
    chunk = rows * cores
    key, value = ret_query_weight.shape[1] // cores, ret_value_weight.shape[1] // cores
    place = jnp.stack([chip, core]).astype(jnp.int32)

    peers = cores * tp
    shard = fox_key_weight.shape[0]
    packed_rows = (3 * cores + 1) * shard
    mine, theirs, sent = pl.pallas_call(
        pack_kernel,
        out_shape=(
            jax.ShapeDtypeStruct((packed_rows, 2 * value), bf16),
            jax.ShapeDtypeStruct((packed_rows, 2 * value), bf16),
            jax.ShapeDtypeStruct((peers, rows, width), bf16),
        ),
        grid=(1,),
        in_specs=[SMEM, whole(rows, width)]
        + [whole(shard, size * cores) for size in (value,) * 6 + (key,) * 2],
        out_specs=(VMEM, VMEM, HBM),
        scratch_shapes=[pltpu.SemaphoreType.DMA((peers,))],
        name="pack",
    )(
        place[1:],
        tokens,
        ret_out_weight.T,
        fox_out_weight.T,
        fox_key_weight,
        fox_value_weight,
        fox_query_weight,
        ret_value_weight,
        ret_key_weight,
        ret_query_weight,
    )
    wide = lax.all_to_all(sent, CHIP, 0, 0, tiled=True)

    got = lax.ppermute(theirs, "sp_1", [(0, 1), (1, 0)])
    packed = (mine.astype(f32) + got.astype(f32)).astype(f16)
    weights = lax.all_gather(packed, "sp_0", axis=0, tiled=True).astype(f32).astype(bf16)
    weights = weights.reshape(-1, packed_rows, 2 * value)
    *parts, payload = pl.pallas_call(
        lambda *refs: project_kernel(*refs, key=key, cores=cores),
        out_shape=(
            jax.ShapeDtypeStruct((chunk, 2 * value), bf16),
            jax.ShapeDtypeStruct((chunk, value), bf16),
            jax.ShapeDtypeStruct((chunk, key), bf16),
            jax.ShapeDtypeStruct((chunk, key), bf16),
            jax.ShapeDtypeStruct((chunk + key, 2 * value), f32),
        ),
        in_specs=[SMEM, SMEM, VMEM, VMEM, VMEM],
        out_specs=(VMEM,) * 5,
        compiler_params=pltpu.CompilerParams(vmem_limit_bytes=20 * MIB),
        name="project",
    )(
        place,
        ret_decay,
        wide.reshape(-1, width),
        norm_gain.reshape(tp, 1, width),
        weights,
    )

    out_rows = weights[:, : shard * cores, :].reshape(-1, 2 * value)
    sent = jnp.broadcast_to(out_rows[None], (peers, *out_rows.shape))
    out_weights = lax.all_to_all(sent, CHIP, 0, 0, tiled=True)

    gathered = lax.all_gather(payload.astype(f16), "sp_0", axis=0, tiled=False)
    gathered = gathered.astype(f32).astype(bf16)

    mix = kernel(
        lambda *refs: mix_kernel(*refs, key=key),
        jax.ShapeDtypeStruct((chunk, 2 * value), bf16),
        [SMEM, SMEM] + [VMEM] * 8,
        24,
    )(
        place,
        ret_decay,
        *parts,
        gathered,
        fox_gates.T,
        ret_state,
        head_norm_gain[None],
    )

    final = rows // tp
    mixes = lax.all_to_all(mix.reshape(cores * tp, final, -1), CHIP, 0, 0, tiled=True)
    return pl.pallas_call(
        lambda *refs: output_kernel(*refs, cores=cores),
        out_shape=jax.ShapeDtypeStruct((final, out_weights.shape[1]), bf16),
        in_specs=[VMEM, HBM],
        out_specs=VMEM,
        scratch_shapes=[
            pltpu.VMEM(out_weights.shape, bf16),
            pltpu.SemaphoreType.DMA((peers,)),
        ],
        compiler_params=pltpu.CompilerParams(vmem_limit_bytes=16 * MIB),
        name="output",
    )(mixes, out_weights)


def solution(mesh):
    torus = Mesh(
        mesh.devices.reshape(mesh.shape["grp"], mesh.shape["sp"] // 2, 2, mesh.shape["tp"]),
        ("grp", "sp_0", "sp_1", "tp"),
    )
    return jax.shard_map(
        layer,
        mesh=torus,
        in_specs=(
            P(GRP_SP, "tp"),
            P(),
            P(SP, "tp"),
            P(SP, "tp"),
            P(SP, "tp"),
            P(SP, "tp"),
            P(SP, "tp"),
            P(SP, "tp"),
            P("tp"),
            P(("grp", "tp"), None, None),
            P("tp"),
            P("grp", "tp"),
            P("tp", SP),
            P("tp", SP),
        ),
        out_specs=P(GRP_SP_TP, None),
        check_vma=False,
    )
```

```python
import jax
import jax.numpy as jnp
from jax import lax
from jax.experimental import pallas as pl
from jax.experimental.pallas import tpu as pltpu
from jax.sharding import Mesh
from jax.sharding import PartitionSpec as P


SP = ("sp_0", "sp_1")
CHIP = ("sp_1", "tp")
GRP_SP = ("grp", "sp_0", "sp_1")
GRP_SP_TP = ("grp", "sp_0", "sp_1", "tp")

EPSILON = 1e-06
LOG2E = 1.4426950408889634
MIB = 2**20

SMALL_WEIGHT = 2.0**18
QUERY_WEIGHT = 2.0**12
FOX_OUT_WEIGHT = 2.0**15
KEY_VALUE = 2.0**7
STATE = 2.0**-9
STATE_LOW = 2.0**8

VMEM = pl.BlockSpec(memory_space=pltpu.VMEM)
SMEM = pl.BlockSpec(memory_space=pltpu.SMEM)
HBM = pl.BlockSpec(memory_space=pltpu.HBM)
NT = (((1,), (1,)), ((), ()))
TN = (((0,), (0,)), ((), ()))


def dot(a, b, dims=(((1,), (0,)), ((), ()))):
    return lax.dot_general(a, b, dims, preferred_element_type=jnp.float32)


def two_terms(x):
    high = x.astype(jnp.bfloat16)
    return high, (x - high.astype(jnp.float32)).astype(jnp.bfloat16)


def column_of(count):
    return lax.broadcasted_iota(jnp.int32, (count, 1), 0).astype(jnp.float32)


def copies(source, target, signals):
    return [
        pltpu.make_async_copy(source, target.at[k], signals.at[k]) for k in range(target.shape[0])
    ]


def arrivals(source, target, signals):
    return [
        pltpu.make_async_copy(source.at[k], target.at[k], signals.at[k])
        for k in range(target.shape[0])
    ]


def pack_kernel(
    core, tokens, out_ret, out_fox, fk, fv, fq, rv, rk, rq, mine, theirs, sent, signals
):
    f32 = jnp.float32
    heads = 2
    started = copies(tokens, sent, signals)
    for copy in started:
        copy.start()

    def columns(ref, h, scale):
        size = ref.shape[1] // heads
        return ref[...].astype(f32)[:, h * size : (h + 1) * size] * scale

    groups = (
        ((out_ret, SMALL_WEIGHT), (out_fox, FOX_OUT_WEIGHT)),
        ((fk, SMALL_WEIGHT), (fv, SMALL_WEIGHT)),
        ((fq, QUERY_WEIGHT), (rv, SMALL_WEIGHT)),
        ((rk, SMALL_WEIGHT), (rq, SMALL_WEIGHT)),
    )
    both = [
        [jnp.concatenate([columns(ref, h, scale) for ref, scale in group], axis=1) for group in groups]
        for h in range(heads)
    ]
    first = core[0] == 0
    shard = both[0][0].shape[0]
    for c in range(heads):
        for g in range(3):
            at = slice((g * heads + c) * shard, (g * heads + c + 1) * shard)
            mine[at, :] = jnp.where(core[0] == c, both[c][g], 0.0).astype(mine.dtype)
            theirs[at, :] = jnp.where(core[0] == c, both[1 - c][g], 0.0).astype(theirs.dtype)
    at = slice(3 * heads * shard, (3 * heads + 1) * shard)

    def halves(left, right):
        left, right = jnp.where(first, left, 0.0), jnp.where(first, 0.0, right)
        return jnp.concatenate([left, right], axis=1)

    mine[at, :] = halves(both[0][3], both[1][3]).astype(mine.dtype)
    theirs[at, :] = halves(both[1][3], both[0][3]).astype(theirs.dtype)
    for copy in started:
        copy.wait()


def project_kernel(
    place,
    decays,
    arrived,
    gains,
    weights,
    query,
    values,
    keys,
    queries,
    payload,
    tokens,
    signals,
    *,
    key,
    cores,
):
    f32, bf16 = jnp.float32, jnp.bfloat16
    rows, width = tokens.shape[1:]
    parts, value = gains.shape[0], 2 * key
    arriving = arrivals(arrived, tokens, signals)
    for copy in arriving:
        copy.start()
    per = weights.shape[0] // parts
    side = width // per
    blocks = []
    for k in range(parts):
        at = slice(k * per, (k + 1) * per)
        pair = weights[at, side : 2 * side, :].reshape(width, 2 * value)
        mixed = weights[at, 2 * side : 3 * side, :].reshape(width, 2 * value)
        last = weights[at, 3 * side :, :]
        last = jnp.concatenate([last[:, :, :value], last[:, :, value:]], axis=1)
        blocks.append((pair, mixed, last.reshape(width, value)))
    factors = []
    for c in range(cores):
        square = jnp.zeros((rows, 1), f32)
        for k in range(parts):
            arriving[c * parts + k].wait()
            x = tokens[c * parts + k].astype(f32)
            square = square + jnp.sum(x * x, axis=1, keepdims=True)
        factors.append(lax.rsqrt(square * (1.0 / (parts * width)) + EPSILON))
    for c in range(cores):
        sums = [jnp.zeros((rows, block.shape[1]), f32) for block in blocks[0]]
        for k in range(parts):
            x = tokens[c * parts + k].astype(f32)
            normed = (x * factors[c] * gains[k]).astype(bf16)
            sums = [total + dot(normed, block) for total, block in zip(sums, blocks[k])]
        pair, mixed, last = sums
        lane = lax.broadcasted_iota(jnp.int32, (rows, 2 * value), 1)
        back = jnp.where(lane < value, 1.0 / QUERY_WEIGHT, 1.0 / SMALL_WEIGHT)
        pair = (pair * (1.0 / SMALL_WEIGHT)).astype(bf16)
        mixed = (mixed * back).astype(bf16)
        last = (last * (1.0 / SMALL_WEIGHT)).astype(bf16)
        at = slice(c * rows, (c + 1) * rows)
        payload[at, :] = pair.astype(f32) * KEY_VALUE
        query[at, :] = jnp.where(lane < value, mixed.astype(f32), 0.0).astype(bf16)
        values[at, :] = mixed[:, value:]
        keys[at, :] = last[:, :key]
        queries[at, :] = last[:, key:]
    chunk = rows * cores
    trailing = jnp.exp((chunk - 1.0 - column_of(chunk)) * decays[place[1]]) * key ** (-0.5)
    high, low = two_terms(keys[...].astype(f32) * trailing)
    summary = (dot(high, values[...], TN) + dot(low, values[...], TN)) * STATE
    high = summary.astype(bf16).astype(f32)
    payload[chunk:, :] = jnp.concatenate([high, (summary - high) * STATE_LOW], axis=1)


def mix_kernel(place, decays, query, values, keys, queries, gathered, gates, state, gains, mix, *, key):
    f32, bf16 = jnp.float32, jnp.bfloat16
    chunk, value = query.shape[0], 2 * key
    own, head = place[0], place[1]
    decay = decays[head]
    attending = query[...]
    scale = value ** (-0.5) * LOG2E / KEY_VALUE

    def gates_of(j):
        pair = gates[:, pl.ds(pl.multiple_of(j * chunk, chunk), chunk)]
        return jnp.where(head == 0, pair[:1], pair[1:])

    base = jnp.max(gates_of(own), axis=1, keepdims=True)

    def logits_of(j):
        pairs = gathered[j, :chunk, :]
        return dot(attending, pairs, NT) * scale - (gates_of(j) - base) * LOG2E, pairs

    row = lax.broadcasted_iota(jnp.int32, (chunk, chunk), 0)
    col = lax.broadcasted_iota(jnp.int32, (chunk, chunk), 1)
    t, pairs = logits_of(own)
    t = jnp.where(col <= row, t, -jnp.inf)
    top = jnp.max(t, axis=1, keepdims=True)
    p = jnp.exp2(t - top)
    total = jnp.sum(p, axis=1, keepdims=True)
    mixed = dot(p.astype(bf16), pairs)

    ones = jnp.ones((1, 2 * value), f32)
    per_chunk = jnp.exp(ones * (chunk * decay))

    def step(j, carry):
        top, total, mixed, memory = carry
        t, pairs = logits_of(j)
        new = jnp.maximum(top, jnp.max(t, axis=1, keepdims=True))
        p = jnp.exp2(t - new)
        keep = jnp.exp2(top - new)
        total = total * keep + jnp.sum(p, axis=1, keepdims=True)
        mixed = mixed * keep + dot(p.astype(bf16), pairs)
        memory = memory * per_chunk + gathered[j, chunk:, :].astype(f32)
        return new, total, mixed, memory

    memory = jnp.zeros((key, 2 * value), f32)
    _, total, mixed, memory = lax.fori_loop(0, own, step, (top, total, mixed, memory))
    fox = (mixed * (1.0 / KEY_VALUE) / total)[:, value:]

    memory = (memory[:, :value] + memory[:, value:] * (1.0 / STATE_LOW)) * (1.0 / STATE)
    first = (own * chunk).astype(f32)
    entering = jnp.exp(ones[:, :value] * (first * decay)) * state[head] + memory
    ret_query = queries[...]
    spread = (row - col).astype(f32)
    within = jnp.where(col <= row, jnp.exp(jnp.maximum(spread, 0.0) * decay), 0.0)
    near = dot(ret_query, keys[...], NT) * within * key ** (-0.5)
    high, low = two_terms(entering)
    carried = dot(ret_query, high) + dot(ret_query, low)
    raw = dot(near.astype(bf16), values[...]) + carried * jnp.exp((column_of(chunk) + 1.0) * decay)
    center = raw - jnp.mean(raw, axis=1, keepdims=True)
    variance = jnp.mean(center * center, axis=1, keepdims=True)
    gain = jnp.where(head == 0, gains[:, :value], gains[:, value:])
    ret = center * lax.rsqrt(variance + EPSILON) * gain
    joined = [ret * (1.0 / SMALL_WEIGHT), fox * (1.0 / FOX_OUT_WEIGHT)]
    mix[...] = jnp.concatenate(joined, axis=1).astype(bf16)


def output_kernel(mixes, stored, out, weights, signals, *, cores):
    parts = mixes.shape[0] // cores
    arriving = arrivals(stored, weights, signals)
    for k in range(parts):
        for c in range(cores):
            arriving[c * parts + k].start()
    summed = jnp.zeros(out.shape, jnp.float32)
    for k in range(parts):
        for c in range(cores):
            arriving[c * parts + k].wait()
        partial = sum(
            dot(mixes[c * parts + k], weights[c * parts + k], NT) for c in range(cores)
        )
        summed = summed + partial.astype(jnp.bfloat16).astype(jnp.float32)
    out[...] = summed.astype(out.dtype)


def kernel(body, out_shape, in_specs, limit):
    return pl.pallas_call(
        body,
        out_shape=out_shape,
        in_specs=in_specs,
        out_specs=VMEM,
        compiler_params=pltpu.CompilerParams(vmem_limit_bytes=limit * MIB),
    )


def whole(*shape):
    return pl.BlockSpec(shape, lambda i: (0,) * len(shape))


def layer(
    tokens,
    norm_gain,
    ret_query_weight,
    ret_key_weight,
    ret_value_weight,
    fox_query_weight,
    fox_key_weight,
    fox_value_weight,
    ret_decay,
    ret_state,
    head_norm_gain,
    fox_gates,
    ret_out_weight,
    fox_out_weight,
):
    f32, bf16, f16 = jnp.float32, jnp.bfloat16, jnp.float16
    chip, core = lax.axis_index("sp_0"), lax.axis_index("sp_1")
    cores, tp = lax.axis_size("sp_1"), lax.axis_size("tp")
    rows, width = tokens.shape
    chunk = rows * cores
    key, value = ret_query_weight.shape[1] // cores, ret_value_weight.shape[1] // cores
    place = jnp.stack([chip, core]).astype(jnp.int32)

    peers = cores * tp
    shard = fox_key_weight.shape[0]
    packed_rows = (3 * cores + 1) * shard
    mine, theirs, sent = pl.pallas_call(
        pack_kernel,
        out_shape=(
            jax.ShapeDtypeStruct((packed_rows, 2 * value), bf16),
            jax.ShapeDtypeStruct((packed_rows, 2 * value), bf16),
            jax.ShapeDtypeStruct((peers, rows, width), bf16),
        ),
        grid=(1,),
        in_specs=[SMEM, whole(rows, width)]
        + [whole(shard, size * cores) for size in (value,) * 6 + (key,) * 2],
        out_specs=(VMEM, VMEM, HBM),
        scratch_shapes=[pltpu.SemaphoreType.DMA((peers,))],
        name="pack",
    )(
        place[1:],
        tokens,
        ret_out_weight.T,
        fox_out_weight.T,
        fox_key_weight,
        fox_value_weight,
        fox_query_weight,
        ret_value_weight,
        ret_key_weight,
        ret_query_weight,
    )
    wide = lax.all_to_all(sent, CHIP, 0, 0, tiled=True)

    got = lax.ppermute(theirs, "sp_1", [(0, 1), (1, 0)])
    packed = (mine.astype(f32) + got.astype(f32)).astype(f16)
    weights = lax.all_gather(packed, "sp_0", axis=0, tiled=True).astype(f32).astype(bf16)
    weights = weights.reshape(-1, packed_rows, 2 * value)
    *parts, payload = pl.pallas_call(
        lambda *refs: project_kernel(*refs, key=key, cores=cores),
        out_shape=(
            jax.ShapeDtypeStruct((chunk, 2 * value), bf16),
            jax.ShapeDtypeStruct((chunk, value), bf16),
            jax.ShapeDtypeStruct((chunk, key), bf16),
            jax.ShapeDtypeStruct((chunk, key), bf16),
            jax.ShapeDtypeStruct((chunk + key, 2 * value), f32),
        ),
        in_specs=[SMEM, SMEM, HBM, VMEM, VMEM],
        out_specs=(VMEM,) * 5,
        scratch_shapes=[
            pltpu.VMEM(wide.shape, bf16),
            pltpu.SemaphoreType.DMA((peers,)),
        ],
        compiler_params=pltpu.CompilerParams(vmem_limit_bytes=20 * MIB),
        name="project",
    )(
        place,
        ret_decay,
        wide,
        norm_gain.reshape(tp, 1, width),
        weights,
    )

    out_rows = weights[:, : shard * cores, :].reshape(-1, 2 * value)
    sent = jnp.broadcast_to(out_rows[None], (peers, *out_rows.shape))
    out_weights = lax.all_to_all(sent, CHIP, 0, 0, tiled=True)

    gathered = lax.all_gather(payload.astype(f16), "sp_0", axis=0, tiled=False)
    gathered = gathered.astype(f32).astype(bf16)

    mix = kernel(
        lambda *refs: mix_kernel(*refs, key=key),
        jax.ShapeDtypeStruct((chunk, 2 * value), bf16),
        [SMEM, SMEM] + [VMEM] * 8,
        24,
    )(
        place,
        ret_decay,
        *parts,
        gathered,
        fox_gates.T,
        ret_state,
        head_norm_gain[None],
    )

    final = rows // tp
    mixes = lax.all_to_all(mix.reshape(cores * tp, final, -1), CHIP, 0, 0, tiled=True)
    return pl.pallas_call(
        lambda *refs: output_kernel(*refs, cores=cores),
        out_shape=jax.ShapeDtypeStruct((final, out_weights.shape[1]), bf16),
        in_specs=[VMEM, HBM],
        out_specs=VMEM,
        scratch_shapes=[
            pltpu.VMEM(out_weights.shape, bf16),
            pltpu.SemaphoreType.DMA((peers,)),
        ],
        compiler_params=pltpu.CompilerParams(vmem_limit_bytes=16 * MIB),
        name="output",
    )(mixes, out_weights)


def solution(mesh):
    torus = Mesh(
        mesh.devices.reshape(mesh.shape["grp"], mesh.shape["sp"] // 2, 2, mesh.shape["tp"]),
        ("grp", "sp_0", "sp_1", "tp"),
    )
    return jax.shard_map(
        layer,
        mesh=torus,
        in_specs=(
            P(GRP_SP, "tp"),
            P(),
            P(SP, "tp"),
            P(SP, "tp"),
            P(SP, "tp"),
            P(SP, "tp"),
            P(SP, "tp"),
            P(SP, "tp"),
            P("tp"),
            P(("grp", "tp"), None, None),
            P("tp"),
            P("grp", "tp"),
            P("tp", SP),
            P("tp", SP),
        ),
        out_specs=P(GRP_SP_TP, None),
        check_vma=False,
    )
```
